32 devices in a mesh: sp: 16 (over z, y, x), tp: 2 (over core).
Axes of the slice: x: 2, y: 2, z: 4, core: 2. Of those that a mesh axis runs over, the one named last changes fastest.
Arguments:
- tokens: bfloat16 [1024, 1, 2048], P('sp'), may hold values from -6 to 6
- queries: bfloat16 [1024, 1, 1024], P('sp', None, 'tp'), may hold values from -15 to 15
- key_values: bfloat16 [1024, 1, 1024], P('sp', None, 'tp'), may hold values from -6 to 6
- stop_bias: bfloat16 [1024, 1, 16], P('sp', None, 'tp'), may hold values from -20 to 0
- out_proj: bfloat16 [1024, 2048], P('tp'), may hold values from -0.375 to 0.375
- norm_gain: float32 [2048], replicated, may hold values from 0.1 to 1.9
- up_proj: bfloat16 [2048, 4096], P('sp', 'tp'), may hold values from -0.125 to 0.125
- down_proj: bfloat16 [4096, 2048], P('tp', 'sp'), may hold values from -0.09375 to 0.09375
Outputs:
- layer_out: bfloat16 [1024, 1, 2048], P(('sp', 'tp'))
The draws below stay inside these ranges and needn't reach their ends.
All inputs are finite; a program needn't handle non-finite values.
Results may differ from the reference program's by a relative error of at most 0.018.
Values may be sent and summed in bfloat16 or wider, within the bound.
A program may use at most 64 MiB of HBM per device.

```python
import jax
import jax.numpy as jnp
from jax import lax

D = 2048
FF = 4096
QUERY_HEAD_COUNT = 16
KV_HEADS = 8
HEAD = 64
SEQUENCE_COUNT = 1
TOK_DEV = 64
TOKEN_LENGTH = 1024
N_TP = 2


def draw_stop_bias(key, part):
    key_tensor = jax.random.split(key, 7)
    fast_heads = jax.random.randint(key_tensor[0], (SEQUENCE_COUNT, QUERY_HEAD_COUNT), 0, 2) == 0
    slow_level = -jnp.log(jnp.float32(TOKEN_LENGTH)) - jax.random.uniform(key_tensor[1], (SEQUENCE_COUNT, QUERY_HEAD_COUNT), minval=2.5, maxval=4.0)
    fast_level = -jax.random.uniform(key_tensor[2], (SEQUENCE_COUNT, QUERY_HEAD_COUNT), minval=6.0, maxval=7.5)
    base_level = jnp.where(fast_heads, fast_level, slow_level)
    block_count = TOKEN_LENGTH // TOK_DEV
    shifts = jax.random.uniform(key_tensor[3], (SEQUENCE_COUNT, QUERY_HEAD_COUNT, block_count), minval=-0.7, maxval=0.7)
    shifts = jnp.repeat(shifts, TOK_DEV, axis=2)
    rough_part = jax.random.uniform(key_tensor[4], (SEQUENCE_COUNT, QUERY_HEAD_COUNT, TOKEN_LENGTH), minval=-1.0, maxval=1.0)
    tier_levels = base_level[:, :, None] + shifts + rough_part
    stretch_places = jax.random.randint(key_tensor[5], (SEQUENCE_COUNT, QUERY_HEAD_COUNT, 4), 0, TOKEN_LENGTH)
    stretch_matches = jnp.any(jnp.arange(TOKEN_LENGTH)[None, None, :, None] == stretch_places[:, :, None, :], axis=3)
    stretch_groups = jax.random.uniform(key_tensor[6], (SEQUENCE_COUNT, QUERY_HEAD_COUNT, TOKEN_LENGTH), minval=-2.0, maxval=0.0)
    tier_levels = jnp.where(stretch_matches, stretch_groups, tier_levels)
    return jnp.transpose(tier_levels, (2, 0, 1)).astype(jnp.float32).astype(jnp.bfloat16)


def steps_of(key, shape, cuts, smallest, high):
    def one(axis_at, shards_of):
        heights = jax.random.uniform(jax.random.fold_in(jax.random.fold_in(key, 6), axis_at), (shards_of,), jnp.float32, smallest / len(cuts), high / len(cuts))
        return jnp.repeat(jnp.exp(heights), shape[axis_at] // shards_of).reshape((-1,) + (1,) * (len(shape) - axis_at - 1))

    level = one(*cuts[0])
    for cut in cuts[1:]:
        level = level * one(*cut)
    return level


def normal_values(stream_key, extent, scale, most, cuts=(), kind=jnp.bfloat16):
    values = jax.random.normal(stream_key, extent, jnp.float32) * scale
    if len(cuts) > 0:
        values = steps_of(stream_key, extent, cuts, -0.22, 0.18) * values
    return jnp.clip(values, min=-most, max=most).astype(kind)


def setup_inputs(seed: int = 0) -> dict:
    seeds = jax.random.split(jax.random.key(seed), 9)
    tokens = normal_values(seeds[0], (TOKEN_LENGTH, SEQUENCE_COUNT, D), 1.0, 6.0, ((0, 16),))
    queries = normal_values(seeds[1], (TOKEN_LENGTH, SEQUENCE_COUNT, QUERY_HEAD_COUNT * HEAD), 2.5, 15.0, ((0, 16), (2, 2)))
    key_values = normal_values(seeds[2], (TOKEN_LENGTH, SEQUENCE_COUNT, KV_HEADS * 2 * HEAD), 1.0, 6.0, ((0, 16), (2, 2)))
    stop_bias = draw_stop_bias(jax.random.fold_in(seeds[8], 71), 0)
    out_proj = normal_values(seeds[4], (QUERY_HEAD_COUNT * HEAD, D), (QUERY_HEAD_COUNT * HEAD // 4) ** -0.5, 0.375, ((0, 2),))
    norm_gain = jnp.clip(1.0 + 0.18 * jax.random.normal(seeds[5], (D,), jnp.float32), 0.1, 1.9)
    up_proj = normal_values(seeds[6], (D, FF), D ** -0.5, 0.125, ((0, 16), (1, 2)))
    down_proj = normal_values(seeds[7], (FF, D), FF ** -0.5, 0.09375, ((0, 2), (1, 16)))
    return {"tokens": tokens, "queries": queries, "key_values": key_values, "stop_bias": stop_bias, "out_proj": out_proj, "norm_gain": norm_gain, "up_proj": up_proj, "down_proj": down_proj}


EPSILON = 1e-06

def rms_scale(residual, gain):
    values = residual.astype(jnp.float32)
    factor = lax.rsqrt(lax.optimization_barrier(jnp.mean(values * values, axis=-1, keepdims=True)) + EPSILON)
    return (values * factor * gain).astype(jnp.bfloat16)

def reference(tokens, queries, key_values, stop_bias, out_proj, norm_gain, up_proj, down_proj):
    total_rows = tokens.shape[0]
    seq_count = tokens.shape[1]
    group_size = QUERY_HEAD_COUNT // KV_HEADS
    block_count = total_rows // TOK_DEV
    query_heads = queries.reshape(total_rows, seq_count, QUERY_HEAD_COUNT, HEAD).transpose(1, 2, 0, 3)
    query_heads = query_heads.reshape(seq_count * QUERY_HEAD_COUNT, total_rows, HEAD)
    kv_pairs = key_values.reshape(total_rows, seq_count, KV_HEADS, 2 * HEAD).transpose(1, 2, 0, 3)
    biases = jnp.transpose(stop_bias, (1, 2, 0)).astype(jnp.float32)
    positions = jnp.arange(total_rows, dtype=jnp.int32)

    def one_head(inputs):
        flat_index, q_head = inputs
        seq_index = flat_index // QUERY_HEAD_COUNT
        head_index = flat_index % QUERY_HEAD_COUNT
        kv_pair = kv_pairs[seq_index, head_index // group_size]
        keys_part = kv_pair[:, :HEAD]
        values_part = kv_pair[:, HEAD:]
        bias_row = biases[seq_index, head_index]
        q_blocks = q_head.reshape(block_count, TOK_DEV, HEAD)

        def one_block(block_inputs):
            number, q_block = block_inputs
            scores = jnp.dot(q_block, jnp.transpose(keys_part), preferred_element_type=jnp.float32) * 0.125 + bias_row[None, :]
            query_pos = number * TOK_DEV + jnp.arange(TOK_DEV, dtype=jnp.int32)
            strict = positions[None, :] < query_pos[:, None]
            log_pass = jnp.where(strict, jax.nn.log_sigmoid(-scores), 0.0)
            after_sum = lax.cumsum(log_pass, axis=1, reverse=True) - log_pass
            weights = jnp.where(strict, jnp.exp(jax.nn.log_sigmoid(scores) + after_sum), 0.0).astype(jnp.bfloat16)
            return jnp.dot(weights, values_part, preferred_element_type=jnp.float32).astype(jnp.bfloat16)
        outputs = lax.map(one_block, (jnp.arange(block_count, dtype=jnp.int32), q_blocks))
        return outputs.reshape(total_rows, HEAD)
    attended = lax.map(one_head, (jnp.arange(seq_count * QUERY_HEAD_COUNT, dtype=jnp.int32), query_heads))
    attended = attended.reshape(seq_count, QUERY_HEAD_COUNT, total_rows, HEAD).transpose(2, 0, 1, 3)
    attended = attended.reshape(total_rows * seq_count, QUERY_HEAD_COUNT * HEAD)
    head_width = QUERY_HEAD_COUNT * HEAD // N_TP
    projected = jnp.zeros((total_rows * seq_count, D), jnp.float32)
    for group_index in range(N_TP):
        lower = group_index * head_width
        partial_value = jnp.dot(attended[:, lower:lower + head_width], out_proj[lower:lower + head_width], preferred_element_type=jnp.float32)
        projected = projected + lax.optimization_barrier(partial_value.astype(jnp.bfloat16)).astype(jnp.float32)
    flat_tokens = tokens.reshape(total_rows * seq_count, D)
    residual = (flat_tokens.astype(jnp.float32) + projected).astype(jnp.bfloat16)
    normed = rms_scale(residual, norm_gain)
    hidden = jnp.square(jax.nn.relu(jnp.dot(normed, up_proj, preferred_element_type=jnp.float32))).astype(jnp.bfloat16)
    unit_width = FF // N_TP
    update = jnp.zeros((total_rows * seq_count, D), jnp.float32)
    for group_index in range(N_TP):
        lower = group_index * unit_width
        partial_value = jnp.dot(hidden[:, lower:lower + unit_width], down_proj[lower:lower + unit_width], preferred_element_type=jnp.float32)
        update = update + lax.optimization_barrier(partial_value.astype(jnp.bfloat16)).astype(jnp.float32)
    result = (residual.astype(jnp.float32) + update).astype(jnp.bfloat16)
    return result.reshape(total_rows, seq_count, D)
```

```python
import math

import jax
import jax.numpy as jnp
from jax import lax
from jax.experimental import pallas as pl
from jax.experimental.pallas import tpu as pltpu
from jax.sharding import PartitionSpec as P

HEAD = 64


EPSILON = 1e-06


def rms_scale(residual, gain):
    values = residual.astype(jnp.float32)
    factor = lax.rsqrt(jnp.mean(values * values, axis=-1, keepdims=True) + EPSILON)
    return (values * factor * gain).astype(jnp.bfloat16)


def sweep_keys(totals, pieces, shard_rows, step_fn):
    kv_rows, bias_rows = pieces
    shards = kv_rows.shape[0] // shard_rows
    group_shards = math.gcd(shards, max(1, 1024 // shard_rows))
    span_rows = group_shards * shard_rows

    def advance(number, running):
        first_row = number * span_rows
        kv_block = lax.dynamic_slice_in_dim(kv_rows, first_row, span_rows, 0)
        bias_block = lax.dynamic_slice_in_dim(bias_rows, first_row, span_rows, 0)
        return step_fn(running, kv_block, bias_block, first_row, group_shards)

    return lax.fori_loop(0, shards // group_shards, advance, totals)


def general_body(tokens, queries, key_values, stop_bias, out_proj, norm_gain, up_proj, down_proj):
    row_count = tokens.shape[0]
    seq_count = tokens.shape[1]
    head_count = queries.shape[2] // HEAD
    kv_count = key_values.shape[2] // (2 * HEAD)
    group_size = head_count // kv_count
    n_shards = lax.axis_size("sp")
    query_start = lax.axis_index("sp") * row_count
    query_pos = query_start + lax.iota(jnp.int32, row_count)
    q_heads = queries.reshape(row_count, seq_count, kv_count, group_size, HEAD).transpose(
        1, 2, 3, 0, 4
    )
    q_heads = q_heads.reshape(seq_count, kv_count, group_size * row_count, HEAD)

    def stick_block(kv_block, bias_block, key_start):
        span_rows = kv_block.shape[0]
        key_pairs = kv_block.reshape(span_rows, seq_count, kv_count, 2 * HEAD)
        keys_part = key_pairs[..., :HEAD]
        values_part = key_pairs[..., HEAD:]
        scores = (
            jnp.einsum("bgmd,sbgd->bgms", q_heads, keys_part, preferred_element_type=jnp.float32)
            * 0.125
        )
        bias_float = jnp.transpose(bias_block, (1, 2, 0)).astype(jnp.float32)
        scores = (
            scores.reshape(seq_count, head_count, row_count, span_rows) + bias_float[:, :, None, :]
        )
        key_pos = key_start + lax.iota(jnp.int32, span_rows)
        strict = key_pos[None, :] < query_pos[:, None]
        log_pass = jnp.where(strict, jax.nn.log_sigmoid(-scores), 0.0)
        return (scores, strict, log_pass, values_part)

    def weigh(scores, strict, after_sum, values_part):
        span_rows = scores.shape[3]
        weights = jnp.where(strict, jnp.exp(jax.nn.log_sigmoid(scores) + after_sum), 0.0).astype(
            jnp.bfloat16
        )
        weights = weights.reshape(seq_count, kv_count, group_size * row_count, span_rows)
        return jnp.einsum(
            "bgms,sbgd->bgmd", weights, values_part, preferred_element_type=jnp.float32
        )

    empty_out = jnp.zeros((seq_count, kv_count, group_size * row_count, HEAD), jnp.float32)

    def sum_step(sums_table, kv_block, bias_block, key_start, shard_group):

        def sum_compute(table_in):
            scores, strict, log_pass, values_part = stick_block(kv_block, bias_block, key_start)
            block_sums = log_pass.reshape(
                seq_count, head_count, row_count, shard_group, row_count
            ).sum(axis=4)
            slot_index = key_start // row_count
            current = lax.dynamic_slice_in_dim(table_in, slot_index, shard_group, 0)
            return lax.dynamic_update_slice_in_dim(
                table_in, current + jnp.transpose(block_sums, (3, 0, 1, 2)), slot_index, 0
            )

        return lax.cond(
            key_start < query_start + row_count, sum_compute, lambda table_in: table_in, sums_table
        )

    empty_table = jnp.zeros((n_shards, seq_count, head_count, row_count), jnp.float32)
    sums_table = sweep_keys(
        empty_table,
        (
            lax.all_gather(key_values, "sp", axis=0, tiled=True),
            lax.all_gather(stop_bias, "sp", axis=0, tiled=True),
        ),
        row_count,
        sum_step,
    )
    offsets = lax.cumsum(sums_table, axis=0, reverse=True) - sums_table

    def out_step(outputs, kv_block, bias_block, key_start, shard_group):

        def out_compute(running):
            scores, strict, log_pass, values_part = stick_block(kv_block, bias_block, key_start)
            span_rows = kv_block.shape[0]
            split_pass = log_pass.reshape(seq_count, head_count, row_count, shard_group, row_count)
            within = lax.cumsum(split_pass, axis=4, reverse=True) - split_pass
            carried = lax.dynamic_slice_in_dim(offsets, key_start // row_count, shard_group, 0)
            carried = jnp.transpose(carried, (1, 2, 3, 0))[..., None]
            after_sum = (within + carried).reshape(seq_count, head_count, row_count, span_rows)
            return running + weigh(scores, strict, after_sum, values_part)

        return lax.cond(
            key_start < query_start + row_count, out_compute, lambda running: running, outputs
        )

    accum_out = sweep_keys(
        empty_out,
        (
            lax.all_gather(key_values, "sp", axis=0, tiled=True),
            lax.all_gather(stop_bias, "sp", axis=0, tiled=True),
        ),
        row_count,
        out_step,
    )
    attended = accum_out.reshape(seq_count, kv_count, group_size, row_count, HEAD).transpose(
        3, 0, 1, 2, 4
    )
    attended = attended.reshape(row_count * seq_count, head_count * HEAD).astype(jnp.bfloat16)
    share_tokens = row_count // lax.axis_size("tp")
    share_rows = share_tokens * seq_count
    tp_index = lax.axis_index("tp")
    projected = lax.psum(
        jnp.dot(attended, out_proj, preferred_element_type=jnp.float32).astype(jnp.bfloat16), "tp"
    ).astype(jnp.float32)
    flat_tokens = tokens.reshape(row_count * seq_count, tokens.shape[2])
    residual = (flat_tokens.astype(jnp.float32) + projected).astype(jnp.bfloat16)
    normed = rms_scale(residual, norm_gain)
    residual_share = lax.dynamic_slice_in_dim(residual, tp_index * share_rows, share_rows, 0)
    up_values = jnp.dot(
        normed,
        lax.all_gather(up_proj, "sp", axis=0, tiled=True),
        preferred_element_type=jnp.float32,
    )
    hidden = jnp.square(jax.nn.relu(up_values)).astype(jnp.bfloat16)
    partial_terms = jnp.dot(
        hidden,
        lax.all_gather(down_proj, "sp", axis=1, tiled=True),
        preferred_element_type=jnp.float32,
    )
    update = lax.psum_scatter(
        partial_terms.astype(jnp.bfloat16), "tp", scatter_dimension=0, tiled=True
    ).astype(jnp.float32)
    result = (residual_share.astype(jnp.float32) + update).astype(jnp.bfloat16)
    return result.reshape(share_tokens, seq_count, result.shape[1])


MESH = pl.DeviceIdType.MESH
LO = 4
LANES = 128
F32 = jnp.float32
BF16 = jnp.bfloat16


def remote(src, dst, send, recv, sp, tp):
    return pltpu.make_async_remote_copy(
        src_ref=src,
        dst_ref=dst,
        send_sem=send,
        recv_sem=recv,
        device_id={"sp": sp, "tp": tp},
        device_id_type=MESH,
    )


def dot_nt(a, b):
    return lax.dot_general(a, b, (((1,), (1,)), ((), ())), preferred_element_type=F32)


def dot_tn(a, b):
    return lax.dot_general(a, b, (((0,), (0,)), ((), ())), preferred_element_type=F32)


class Refs:
    def __init__(self, names, refs):
        for name, ref in zip(names, refs):
            setattr(self, name, ref)


class Piece:
    def __init__(self, r, place, view, rows, send, recv, half):
        self.r, self.view, self.rows, self.send, self.recv, self.half = r, view, rows, send, recv, half
        self.s, self.c, self.hi, self.lo, self.lo1, self.lo2, self.lo3 = place

    def full(self, j):
        return self.view(j, 0, self.rows)

    def part(self, j, h):
        return self.view(j, h * (self.rows // 2), self.rows // 2)

    def direct(self, z, src=None):
        j = z * LO + self.lo
        src = self.full(j) if src is None else src
        return [
            remote(src, self.full(j), self.send.at[z * 4 + k], self.recv.at[j], self.hi * LO + p, self.c)
            for k, p in enumerate((self.lo1, self.lo2))
        ]

    def diag(self, z):
        a, b = z * LO + self.lo1, z * LO + self.lo2
        first, last = self.part(a, 0), self.part(b, 1)
        return [
            remote(first, first, self.send.at[z * 4 + 2], self.recv.at[a], self.hi * LO + self.lo2, self.c),
            remote(last, last, self.send.at[z * 4 + 3], self.half.at[z], self.hi * LO + self.lo1, self.c),
        ]

    def arrived(self, ref, sem):
        remote(ref, ref, self.send.at[0], sem, self.s, 1 - self.c).wait_recv()

    def wait_own(self, z):
        j = z * LO + self.lo
        self.arrived(self.full(j), self.recv.at[j])

    def wait_direct(self, z):
        for p in (self.lo1, self.lo2):
            j = z * LO + p
            self.arrived(self.full(j), self.recv.at[j])

    def wait_diag(self, z):
        j = z * LO + self.lo3
        self.arrived(self.part(j, 0), self.recv.at[j])
        self.arrived(self.part(j, 1), self.half.at[z])


def start(copies):
    for copy in copies:
        copy.start()


def layer_kernel(HI, G, NC, names, *refs):
    r = Refs(names, refs)
    s = lax.axis_index("sp")
    c = lax.axis_index("tp")
    hi = s // LO
    lo = s % LO
    lo1 = lo + 1 - 2 * (lo % 2)
    lo2 = (lo + 2) % LO
    lo3 = (lo1 + 2) % LO
    other = 1 - c
    peers = (lo1, lo2, lo3)
    T = r.q_v.shape[0]
    H = T // 2
    D = r.tok_v.shape[1]
    R = r.up_v.shape[0]
    CH = r.up_buf.shape[1]
    W = r.dn_v.shape[1]
    PL = LO * T
    QR = 2 * PL
    own_cols = pl.ds(pl.multiple_of(hi * CH, LANES), CH)
    own_lanes = pl.ds(pl.multiple_of(lo * LANES, LANES), LANES)

    barrier = pltpu.get_barrier_semaphore()
    for p in peers:
        pl.semaphore_signal(barrier, inc=1, device_id={"sp": hi * LO + p, "tp": c}, device_id_type=MESH)
    pl.semaphore_signal(barrier, inc=1, device_id={"sp": s, "tp": other}, device_id_type=MESH)
    for dz in range(1, HI):
        far = ((hi + dz) % HI) * LO + lo
        pl.semaphore_signal(barrier, inc=1, device_id={"sp": far, "tp": c}, device_id_type=MESH)
    local = [
        (r.q_hbm, r.q_v),
        (r.kv_hbm, r.kv_v),
        (r.up_hbm, r.up_v),
        (r.dn_hbm, r.dn_v),
        (r.up_hbm.at[:, own_cols], r.up_buf.at[pl.ds(s * R, R)]),
        (r.dn_hbm.at[pl.ds(hi * CH, CH)], r.dn_buf.at[s]),
        (r.tok_hbm, r.tok_v),
        (r.wo_hbm, r.wo_v),
        (r.gain_hbm, r.gain_v),
    ]
    loads = [pltpu.make_async_copy(a, b, r.load_sem.at[i]) for i, (a, b) in enumerate(local)]
    start(loads)

    half_lane = lax.broadcasted_iota(jnp.int32, (2 * G, LANES), 1) // HEAD
    bias = r.bias_ref[...].astype(F32)
    bias = jnp.where(half_lane == lo % 2, jnp.concatenate([bias, bias], axis=1), 0.0)
    for g in range(G):
        r.bias_out[g] = bias if g == 0 else pltpu.roll(bias, 2 * G - 2 * g, 0)
    for load in loads[:4]:
        load.wait()
    pl.semaphore_wait(barrier, 4 + (HI - 1))

    place = (s, c, hi, lo, lo1, lo2, lo3)
    up = Piece(r, place, lambda j, a, n: r.up_buf.at[pl.ds(j * R + a, n)], R, r.up_sp, r.up_recv, r.up_half)
    dn = Piece(r, place, lambda j, a, n: r.dn_buf.at[j, pl.ds(a, n)], CH, r.dn_sp, r.dn_recv, r.dn_half)

    def arrived(ref, sem):
        remote(ref, ref, r.pj_send, sem, s, other).wait_recv()

    def spread_heads(k, p):
        lanes = pl.ds(pl.multiple_of(p * LANES, LANES), LANES)
        dev = hi * LO + p
        return [
            remote(r.kv_v.at[:, lanes], r.kv_buf.at[hi, pl.ds(lo * T, T)], r.a_send.at[3 * k], r.k_recv.at[lo], dev, c),
            remote(r.q_v.at[:, lanes], r.q_in.at[lo], r.a_send.at[3 * k + 1], r.q_recv.at[lo], dev, c),
            remote(r.bias_out.at[p], r.bias_in.at[lo], r.a_send.at[3 * k + 2], r.b_recv.at[lo], dev, c),
        ]

    def up_far(hp):
        cols = pl.ds(pl.multiple_of(hp * CH, LANES), CH)
        return remote(r.up_v.at[:, cols], up.full(s), r.wz_send.at[2 * hp], r.up_recv.at[s], hp * LO + lo, c)

    def dn_far(hp):
        rows = pl.ds(hp * CH, CH)
        return remote(r.dn_v.at[rows], dn.full(s), r.wz_send.at[2 * hp + 1], r.dn_recv.at[s], hp * LO + lo, c)

    small = jnp.minimum(hi, HI - 1 - hi)
    tilt = jnp.where(hi <= HI - 1 - hi, 1, -1)

    def nth(k):
        if k == 0:
            return hi
        near = hi - (k + 1) // 2 if k % 2 else hi + k // 2
        return jnp.where(k <= 2 * small, near, hi + tilt * (k - small))

    def below(far, d):
        @pl.when(hi >= d)
        def _():
            far(hi - d).start()

    def above(far, d):
        @pl.when(hi + d < HI)
        def _():
            far(hi + d).start()

    for k, p in enumerate(peers):
        start(spread_heads(k, p))
    start(up.direct(hi, r.up_v.at[:, own_cols]))
    start(dn.direct(hi, r.dn_v.at[pl.ds(hi * CH, CH)]))
    for d in range(1, HI):
        below(up_far, d)
    above(up_far, 1)

    r.q_in[lo] = r.q_v[:, own_lanes]
    r.kv_buf[hi, pl.ds(lo * T, T), :] = r.kv_v[:, own_lanes]
    r.bias_in[lo] = r.bias_out[lo]
    row_id = lax.broadcasted_iota(jnp.int32, (PL, PL + LANES), 0)
    col_id = lax.broadcasted_iota(jnp.int32, (PL, PL + LANES), 1)
    after_key = (row_id > col_id) | (col_id >= PL)
    r.tri_buf[...] = jnp.where(after_key, 1.0, 0.0).astype(BF16)
    low = lax.broadcasted_iota(jnp.int32, (T, LANES), 1) < HEAD

    for p in peers:
        arrived(r.kv_buf.at[hi, pl.ds(p * T, T)], r.k_recv.at[p])
        arrived(r.q_in.at[p], r.q_recv.at[p])
        arrived(r.bias_in.at[p], r.b_recv.at[p])
    for i in range(LO // 2):
        r.bias_pl[hi, :, i * LANES : (i + 1) * LANES] = r.bias_in[2 * i] + r.bias_in[2 * i + 1]

    def keys_up(z):
        dev = (hi + 1) * LO + lo
        return [
            remote(r.kv_buf.at[z], r.kv_buf.at[z], r.kz_send.at[2 * z], r.kz_recv.at[z], dev, c),
            remote(r.bias_pl.at[z], r.bias_pl.at[z], r.kz_send.at[2 * z + 1], r.bz_recv.at[z], dev, c),
        ]

    @pl.when(hi + 1 < HI)
    def _():
        start(keys_up(hi))

    for d in range(2, HI):
        above(up_far, d)

    for j in range(LO):
        qg = r.q_in[j].astype(F32) * 0.125
        r.q_all[j * T : (j + 1) * T] = jnp.where(low, qg, 0.0).astype(BF16)
        r.q_all[PL + j * T : PL + (j + 1) * T] = jnp.where(low, pltpu.roll(qg, HEAD, 1), 0.0).astype(BF16)

    step = 128

    def attend(z, own):
        keys = r.kv_buf[z]
        for i in range(QR // step):
            rows = slice(i * step, (i + 1) * step)
            head = i * step // PL
            scores = dot_nt(r.q_all[rows], keys) + r.bias_pl[z, head : head + 1, :]
            soft = jnp.maximum(scores, 0.0) + jnp.log(1.0 + jnp.exp(-jnp.abs(scores)))
            log_pass = -soft
            if own:
                query = i * step % PL + lax.broadcasted_iota(jnp.int32, (step, PL), 0)
                strict = lax.broadcasted_iota(jnp.int32, (step, PL), 1) < query
                log_pass = jnp.where(strict, log_pass, 0.0)
            top = log_pass.astype(BF16)
            rest = (log_pass - top.astype(F32)).astype(BF16)
            sums = jnp.dot(top, r.tri_buf[...], preferred_element_type=F32) + jnp.dot(
                rest, r.tri_buf[...], preferred_element_type=F32
            )
            power = scores - soft + sums[:, :PL]
            if not own:
                held = r.carry[rows]
                power = power + jnp.concatenate([held] * (PL // LANES), axis=1)
            weights = jnp.exp(power)
            if own:
                weights = jnp.where(strict, weights, 0.0)
            part = jnp.dot(weights.astype(BF16), keys, preferred_element_type=F32)
            if own:
                r.acc[rows] = part
                r.carry[rows] = sums[:, PL:]
            else:
                r.acc[rows] += part
                r.carry[rows] = held + sums[:, PL:]

    def look(d):
        @pl.when(hi >= d)
        def _():
            z = hi - d
            arrived(r.kv_buf.at[z], r.kz_recv.at[z])
            arrived(r.bias_pl.at[z], r.bz_recv.at[z])

            @pl.when(hi + 1 < HI)
            def _():
                start(keys_up(z))

            attend(z, False)

    def relay_direct(piece, k):
        piece.wait_own(nth(k))
        start(piece.direct(nth(k)))

    def relay_diag(piece, k):
        piece.wait_direct(nth(k))
        start(piece.diag(nth(k)))

    attend(hi, True)
    relay_diag(up, 0)
    relay_direct(up, 1)
    for d in range(1, HI):
        look(d)
        relay_diag(up, d)
        if d + 1 < HI:
            relay_direct(up, d + 1)

    heads = [r.acc[h * PL : (h + 1) * PL] for h in range(2)]
    low_pl = lax.broadcasted_iota(jnp.int32, (PL, LANES), 1) < HEAD
    r.att_pl[...] = jnp.where(low_pl, pltpu.roll(heads[0], HEAD, 1), heads[1]).astype(BF16)

    def att_back(k, p):
        src = r.att_pl.at[pl.ds(p * T, T)]
        return remote(src, r.att_buf.at[:, own_lanes], r.t_send.at[k], r.t_recv.at[lo], hi * LO + p, c)

    for k, p in enumerate(peers):
        att_back(k, p).start()
    r.att_buf[:, own_lanes] = r.att_pl[pl.ds(lo * T, T), :]
    relay_diag(dn, 0)
    for d in range(1, HI):
        below(dn_far, d)
        above(dn_far, d)
    for load in loads[4:]:
        load.wait()
    for p in peers:
        lanes = pl.ds(pl.multiple_of(p * LANES, LANES), LANES)
        arrived(r.att_buf.at[:, lanes], r.t_recv.at[p])

    att = r.att_buf[...]
    wide = 512 if D % 512 == 0 else LANES
    for i in range(D // wide):
        cols = slice(i * wide, (i + 1) * wide)
        r.pj_buf[:, cols] = jnp.dot(att, r.wo_v[:, cols], preferred_element_type=F32).astype(BF16)
    pj_copy = remote(r.pj_buf.at[pl.ds(other * H, H)], r.pj_in, r.pj_send, r.pj_recv, s, other)
    pj_copy.start()
    pj_copy.wait()
    mine = pl.ds(c * H, H)
    total = r.pj_buf[mine, :].astype(F32) + r.pj_in[...].astype(F32)
    residual = (r.tok_v[mine, :].astype(F32) + total).astype(BF16)
    r.res_buf[...] = residual
    values = residual.astype(F32)
    factor = lax.rsqrt(jnp.mean(values * values, axis=-1, keepdims=True) + EPSILON)
    r.n_buf[pl.ds((c * HI + hi) * H, H), :] = (values * factor * r.gain_v[...]).astype(BF16)

    NW = D // NC

    def n_at(z, core, q):
        return r.n_buf.at[pl.ds((core * HI + z) * H, H), q * NW : (q + 1) * NW]

    def n_up(z, q):
        return remote(n_at(z, c, q), n_at(z, c, q), r.nu_send.at[z * NC + q], r.nz_recv.at[z * NC + q], s + LO, c)

    def n_down(z, q):
        return remote(n_at(z, c, q), n_at(z, c, q), r.nd_send.at[z * NC + q], r.nz_recv.at[z * NC + q], s - LO, c)

    def n_pass(z, q):
        return remote(n_at(z, c, q), n_at(z, c, q), r.np_send.at[z * NC + q], r.nc_recv.at[z * NC + q], s, other)

    for q in range(NC):

        @pl.when(hi + 1 < HI)
        def _():
            n_up(hi, q).start()

        @pl.when(hi > 0)
        def _():
            n_down(hi, q).start()

    for q in range(NC):
        n_pass(hi, q).start()

    def norm_below(d):
        @pl.when(hi >= d)
        def _():
            z = hi - d
            for q in range(NC):
                arrived(n_at(z, c, q), r.nz_recv.at[z * NC + q])

                @pl.when(hi + 1 < HI)
                def _():
                    n_up(z, q).start()

                n_pass(z, q).start()

    def norm_above(d):
        @pl.when(hi + d < HI)
        def _():
            z = hi + d
            for q in range(NC):
                arrived(n_at(z, c, q), r.nz_recv.at[z * NC + q])

                @pl.when(hi > 0)
                def _():
                    n_down(z, q).start()

                n_pass(z, q).start()

    for d in range(1, HI):
        norm_below(d)
    relay_direct(dn, 1)
    for d in range(1, HI):
        norm_above(d)
        if d == 1:
            relay_diag(dn, 1)
            relay_direct(dn, 2)
    for z in range(HI):
        for q in range(NC):
            arrived(n_at(z, other, q), r.nc_recv.at[z * NC + q])
    for k in range(HI):
        up.wait_diag(nth(k))
    relay_diag(dn, 2)

    wide = 256 if CH % 256 == 0 else LANES
    for i in range(CH // wide):
        cols = slice(i * wide, (i + 1) * wide)
        raw = jnp.maximum(jnp.dot(r.n_buf[...], r.up_buf[:, cols], preferred_element_type=F32), 0.0)
        r.hid_buf[:, cols] = (raw * raw).astype(BF16)
    for k in range(3, HI):
        relay_direct(dn, k)

    half = HI * H

    def x_out(k):
        z = nth(k)
        rows = pl.ds(other * half, half)
        return remote(r.ps_buf.at[z, rows], r.x_in.at[z], r.x_send.at[k], r.x_recv.at[z], s, other)

    def p_out(k, far):
        z = nth(k)
        hp = (hi + far) % HI
        return remote(
            r.xs_buf.at[z, pl.ds(hp * H, H)],
            r.pr_buf.at[hi, z],
            r.p_send.at[k * HI + far],
            r.p_recv.at[hi * HI + z],
            hp * LO + lo,
            c,
        )

    def spread(k):
        z = nth(k)
        arrived(r.x_in.at[z], r.x_recv.at[z])
        mixed = r.ps_buf[z, pl.ds(c * half, half), :].astype(F32) + r.x_in[z].astype(F32)
        r.xs_buf[z] = mixed.astype(BF16)
        for far in range(1, HI):
            p_out(k, far).start()

    for k in range(HI):
        if k >= 2 and k + 1 < HI:
            relay_diag(dn, k + 1)
        z = nth(k)
        dn.wait_diag(z)
        for q in range(0, LO, 2):
            pair = jnp.concatenate([r.dn_buf[z * LO + q], r.dn_buf[z * LO + q + 1]], axis=1)
            part = jnp.dot(r.hid_buf[...], pair, preferred_element_type=F32)
            r.ps_buf[z, :, q * W : (q + 2) * W] = part.astype(BF16)
        x_out(k).start()
        if k > 0:
            spread(k - 1)
    spread(HI - 1)
    CW = LO * W
    for k in range(HI):
        z = nth(k)
        cols = pl.ds(pl.multiple_of(z * CW, LANES), CW)
        update = r.xs_buf[z, pl.ds(hi * H, H), :].astype(F32)
        for far in range(1, HI):
            src = (hi + HI - far) % HI
            arrived(r.pr_buf.at[src, z], r.p_recv.at[src * HI + z])
            update = update + r.pr_buf[src, z].astype(F32)
        r.out_ref[:, cols] = (r.res_buf[:, cols].astype(F32) + update).astype(BF16)

    for k, p in enumerate(peers):
        for copy in spread_heads(k, p):
            copy.wait_send()
        att_back(k, p).wait_send()
    for z in range(HI):

        @pl.when(z != hi)
        def _():
            up_far(z).wait_send()
            dn_far(z).wait_send()

        for copy in up.direct(z) + up.diag(z) + dn.direct(z) + dn.diag(z):
            copy.wait_send()

        @pl.when((z <= hi) & (hi + 1 < HI))
        def _():
            for copy in keys_up(z):
                copy.wait_send()
            for q in range(NC):
                n_up(z, q).wait_send()

        @pl.when((z >= hi) & (hi > 0))
        def _():
            for q in range(NC):
                n_down(z, q).wait_send()

        for q in range(NC):
            n_pass(z, q).wait_send()
        x_out(z).wait_send()
        for far in range(1, HI):
            p_out(z, far).wait_send()


def fits(tokens, queries, key_values, stop_bias, up_proj, down_proj):
    sp = lax.axis_size("sp")
    rows, seqs, heads = stop_bias.shape
    hidden = up_proj.shape[1]
    return (
        lax.axis_size("tp") == 2
        and sp % LO == 0
        and sp > LO
        and seqs == 1
        and heads == 2 * LO
        and queries.shape[2] == heads * HEAD
        and key_values.shape[2] == heads * HEAD
        and 2 * HEAD == LANES
        and 2 * rows == LANES
        and hidden % (sp // LO * LANES) == 0
        and down_proj.shape[1] % LANES == 0
        and up_proj.shape[0] % 16 == 0
        and tokens.shape[2] % 512 == 0
    )


def body(tokens, queries, key_values, stop_bias, out_proj, norm_gain, up_proj, down_proj):
    if not fits(tokens, queries, key_values, stop_bias, up_proj, down_proj):
        return general_body(
            tokens, queries, key_values, stop_bias, out_proj, norm_gain, up_proj, down_proj
        )
    sp = lax.axis_size("sp")
    HI = sp // LO
    T, _, D = tokens.shape
    H = T // 2
    heads = stop_bias.shape[2]
    G = heads // 2
    R, hidden = up_proj.shape
    CH = hidden // HI
    W = down_proj.shape[1]
    PL = LO * T
    NC = 4
    vmem = pl.BlockSpec(memory_space=pltpu.VMEM)
    hbm = pl.BlockSpec(memory_space=pl.ANY)

    def sem(*shape):
        return pltpu.SemaphoreType.DMA(shape)

    operands = dict(
        tok_hbm=(tokens.reshape(T, D), hbm),
        q_hbm=(queries.reshape(T, queries.shape[2]), hbm),
        kv_hbm=(key_values.reshape(T, key_values.shape[2]), hbm),
        bias_ref=(stop_bias.reshape(T, heads).T, vmem),
        wo_hbm=(out_proj, hbm),
        gain_hbm=(norm_gain.reshape(1, D), hbm),
        up_hbm=(up_proj, hbm),
        dn_hbm=(down_proj, hbm),
    )
    scratch = dict(
        tok_v=pltpu.VMEM((T, D), BF16),
        q_v=pltpu.VMEM((T, G * LANES), BF16),
        kv_v=pltpu.VMEM((T, G * LANES), BF16),
        wo_v=pltpu.VMEM(out_proj.shape, BF16),
        gain_v=pltpu.VMEM((1, D), F32),
        up_v=pltpu.VMEM((R, hidden), BF16),
        dn_v=pltpu.VMEM((hidden, W), BF16),
        up_buf=pltpu.VMEM((sp * R, CH), BF16),
        dn_buf=pltpu.VMEM((sp, CH, W), BF16),
        bias_out=pltpu.VMEM((G, 2 * G, LANES), F32),
        bias_in=pltpu.VMEM((LO, 2 * G, LANES), F32),
        bias_pl=pltpu.VMEM((HI, 2 * G, PL), F32),
        q_in=pltpu.VMEM((LO, T, LANES), BF16),
        q_all=pltpu.VMEM((2 * PL, LANES), BF16),
        kv_buf=pltpu.VMEM((HI, PL, LANES), BF16),
        tri_buf=pltpu.VMEM((PL, PL + LANES), BF16),
        carry=pltpu.VMEM((2 * PL, LANES), F32),
        acc=pltpu.VMEM((2 * PL, LANES), F32),
        att_pl=pltpu.VMEM((PL, LANES), BF16),
        att_buf=pltpu.VMEM((T, G * LANES), BF16),
        pj_buf=pltpu.VMEM((T, D), BF16),
        pj_in=pltpu.VMEM((H, D), BF16),
        res_buf=pltpu.VMEM((H, D), BF16),
        n_buf=pltpu.VMEM((HI * T, D), BF16),
        hid_buf=pltpu.VMEM((HI * T, CH), BF16),
        ps_buf=pltpu.VMEM((HI, HI * T, LO * W), BF16),
        x_in=pltpu.VMEM((HI, HI * H, LO * W), BF16),
        xs_buf=pltpu.VMEM((HI, HI * H, LO * W), BF16),
        pr_buf=pltpu.VMEM((HI, HI, H, LO * W), BF16),
        load_sem=sem(9),
        a_send=sem(9),
        k_recv=sem(LO),
        q_recv=sem(LO),
        b_recv=sem(LO),
        kz_send=sem(2 * HI),
        kz_recv=sem(HI),
        bz_recv=sem(HI),
        wz_send=sem(HI * 2),
        up_sp=sem(HI * 4),
        up_recv=sem(sp),
        up_half=sem(HI),
        dn_sp=sem(HI * 4),
        dn_recv=sem(sp),
        dn_half=sem(HI),
        t_send=sem(3),
        t_recv=sem(LO),
        pj_send=pltpu.SemaphoreType.DMA,
        pj_recv=pltpu.SemaphoreType.DMA,
        nu_send=sem(HI * NC),
        nd_send=sem(HI * NC),
        np_send=sem(HI * NC),
        nz_recv=sem(HI * NC),
        nc_recv=sem(HI * NC),
        x_send=sem(HI),
        x_recv=sem(HI),
        p_send=sem(HI * HI),
        p_recv=sem(HI * HI),
    )
    names = [*operands, "out_ref", *scratch]
    out = pl.pallas_call(
        lambda *refs: layer_kernel(HI, G, NC, names, *refs),
        out_shape=jax.ShapeDtypeStruct((H, D), BF16),
        in_specs=[spec for _, spec in operands.values()],
        out_specs=vmem,
        scratch_shapes=list(scratch.values()),
        compiler_params=pltpu.CompilerParams(
            collective_id=0, has_side_effects=True, vmem_limit_bytes=56 * 1024 * 1024
        ),
        name="layer",
    )(*[value for value, _ in operands.values()])
    return out.reshape(H, 1, D)


def solution(mesh):
    return jax.shard_map(
        body,
        mesh=mesh,
        in_specs=(
            P("sp", None, None),
            P("sp", None, "tp"),
            P("sp", None, "tp"),
            P("sp", None, "tp"),
            P("tp", None),
            P(),
            P("sp", "tp"),
            P("tp", "sp"),
        ),
        out_specs=P(("sp", "tp"), None, None),
        check_vma=False,
    )
```

```python
import math

import jax
import jax.numpy as jnp
from jax import lax
from jax.experimental import pallas as pl
from jax.experimental.pallas import tpu as pltpu
from jax.sharding import PartitionSpec as P

HEAD = 64


EPSILON = 1e-06


def rms_scale(residual, gain):
    values = residual.astype(jnp.float32)
    factor = lax.rsqrt(jnp.mean(values * values, axis=-1, keepdims=True) + EPSILON)
    return (values * factor * gain).astype(jnp.bfloat16)


def sweep_keys(totals, pieces, shard_rows, step_fn):
    kv_rows, bias_rows = pieces
    shards = kv_rows.shape[0] // shard_rows
    group_shards = math.gcd(shards, max(1, 1024 // shard_rows))
    span_rows = group_shards * shard_rows

    def advance(number, running):
        first_row = number * span_rows
        kv_block = lax.dynamic_slice_in_dim(kv_rows, first_row, span_rows, 0)
        bias_block = lax.dynamic_slice_in_dim(bias_rows, first_row, span_rows, 0)
        return step_fn(running, kv_block, bias_block, first_row, group_shards)

    return lax.fori_loop(0, shards // group_shards, advance, totals)


def general_body(tokens, queries, key_values, stop_bias, out_proj, norm_gain, up_proj, down_proj):
    row_count = tokens.shape[0]
    seq_count = tokens.shape[1]
    head_count = queries.shape[2] // HEAD
    kv_count = key_values.shape[2] // (2 * HEAD)
    group_size = head_count // kv_count
    n_shards = lax.axis_size("sp")
    query_start = lax.axis_index("sp") * row_count
    query_pos = query_start + lax.iota(jnp.int32, row_count)
    q_heads = queries.reshape(row_count, seq_count, kv_count, group_size, HEAD).transpose(
        1, 2, 3, 0, 4
    )
    q_heads = q_heads.reshape(seq_count, kv_count, group_size * row_count, HEAD)

    def stick_block(kv_block, bias_block, key_start):
        span_rows = kv_block.shape[0]
        key_pairs = kv_block.reshape(span_rows, seq_count, kv_count, 2 * HEAD)
        keys_part = key_pairs[..., :HEAD]
        values_part = key_pairs[..., HEAD:]
        scores = (
            jnp.einsum("bgmd,sbgd->bgms", q_heads, keys_part, preferred_element_type=jnp.float32)
            * 0.125
        )
        bias_float = jnp.transpose(bias_block, (1, 2, 0)).astype(jnp.float32)
        scores = (
            scores.reshape(seq_count, head_count, row_count, span_rows) + bias_float[:, :, None, :]
        )
        key_pos = key_start + lax.iota(jnp.int32, span_rows)
        strict = key_pos[None, :] < query_pos[:, None]
        log_pass = jnp.where(strict, jax.nn.log_sigmoid(-scores), 0.0)
        return (scores, strict, log_pass, values_part)

    def weigh(scores, strict, after_sum, values_part):
        span_rows = scores.shape[3]
        weights = jnp.where(strict, jnp.exp(jax.nn.log_sigmoid(scores) + after_sum), 0.0).astype(
            jnp.bfloat16
        )
        weights = weights.reshape(seq_count, kv_count, group_size * row_count, span_rows)
        return jnp.einsum(
            "bgms,sbgd->bgmd", weights, values_part, preferred_element_type=jnp.float32
        )

    empty_out = jnp.zeros((seq_count, kv_count, group_size * row_count, HEAD), jnp.float32)

    def sum_step(sums_table, kv_block, bias_block, key_start, shard_group):

        def sum_compute(table_in):
            scores, strict, log_pass, values_part = stick_block(kv_block, bias_block, key_start)
            block_sums = log_pass.reshape(
                seq_count, head_count, row_count, shard_group, row_count
            ).sum(axis=4)
            slot_index = key_start // row_count
            current = lax.dynamic_slice_in_dim(table_in, slot_index, shard_group, 0)
            return lax.dynamic_update_slice_in_dim(
                table_in, current + jnp.transpose(block_sums, (3, 0, 1, 2)), slot_index, 0
            )

        return lax.cond(
            key_start < query_start + row_count, sum_compute, lambda table_in: table_in, sums_table
        )

    empty_table = jnp.zeros((n_shards, seq_count, head_count, row_count), jnp.float32)
    sums_table = sweep_keys(
        empty_table,
        (
            lax.all_gather(key_values, "sp", axis=0, tiled=True),
            lax.all_gather(stop_bias, "sp", axis=0, tiled=True),
        ),
        row_count,
        sum_step,
    )
    offsets = lax.cumsum(sums_table, axis=0, reverse=True) - sums_table

    def out_step(outputs, kv_block, bias_block, key_start, shard_group):

        def out_compute(running):
            scores, strict, log_pass, values_part = stick_block(kv_block, bias_block, key_start)
            span_rows = kv_block.shape[0]
            split_pass = log_pass.reshape(seq_count, head_count, row_count, shard_group, row_count)
            within = lax.cumsum(split_pass, axis=4, reverse=True) - split_pass
            carried = lax.dynamic_slice_in_dim(offsets, key_start // row_count, shard_group, 0)
            carried = jnp.transpose(carried, (1, 2, 3, 0))[..., None]
            after_sum = (within + carried).reshape(seq_count, head_count, row_count, span_rows)
            return running + weigh(scores, strict, after_sum, values_part)

        return lax.cond(
            key_start < query_start + row_count, out_compute, lambda running: running, outputs
        )

    accum_out = sweep_keys(
        empty_out,
        (
            lax.all_gather(key_values, "sp", axis=0, tiled=True),
            lax.all_gather(stop_bias, "sp", axis=0, tiled=True),
        ),
        row_count,
        out_step,
    )
    attended = accum_out.reshape(seq_count, kv_count, group_size, row_count, HEAD).transpose(
        3, 0, 1, 2, 4
    )
    attended = attended.reshape(row_count * seq_count, head_count * HEAD).astype(jnp.bfloat16)
    share_tokens = row_count // lax.axis_size("tp")
    share_rows = share_tokens * seq_count
    tp_index = lax.axis_index("tp")
    projected = lax.psum(
        jnp.dot(attended, out_proj, preferred_element_type=jnp.float32).astype(jnp.bfloat16), "tp"
    ).astype(jnp.float32)
    flat_tokens = tokens.reshape(row_count * seq_count, tokens.shape[2])
    residual = (flat_tokens.astype(jnp.float32) + projected).astype(jnp.bfloat16)
    normed = rms_scale(residual, norm_gain)
    residual_share = lax.dynamic_slice_in_dim(residual, tp_index * share_rows, share_rows, 0)
    up_values = jnp.dot(
        normed,
        lax.all_gather(up_proj, "sp", axis=0, tiled=True),
        preferred_element_type=jnp.float32,
    )
    hidden = jnp.square(jax.nn.relu(up_values)).astype(jnp.bfloat16)
    partial_terms = jnp.dot(
        hidden,
        lax.all_gather(down_proj, "sp", axis=1, tiled=True),
        preferred_element_type=jnp.float32,
    )
    update = lax.psum_scatter(
        partial_terms.astype(jnp.bfloat16), "tp", scatter_dimension=0, tiled=True
    ).astype(jnp.float32)
    result = (residual_share.astype(jnp.float32) + update).astype(jnp.bfloat16)
    return result.reshape(share_tokens, seq_count, result.shape[1])


MESH = pl.DeviceIdType.MESH
LO = 4
LANES = 128
F32 = jnp.float32
BF16 = jnp.bfloat16


def remote(src, dst, send, recv, sp, tp):
    return pltpu.make_async_remote_copy(
        src_ref=src,
        dst_ref=dst,
        send_sem=send,
        recv_sem=recv,
        device_id={"sp": sp, "tp": tp},
        device_id_type=MESH,
    )


def dot_nt(a, b):
    return lax.dot_general(a, b, (((1,), (1,)), ((), ())), preferred_element_type=F32)


def dot_tn(a, b):
    return lax.dot_general(a, b, (((0,), (0,)), ((), ())), preferred_element_type=F32)


class Refs:
    def __init__(self, names, refs):
        for name, ref in zip(names, refs):
            setattr(self, name, ref)


class Piece:
    def __init__(self, place, view, blocks, rows, sem):
        self.view, self.blocks, self.rows = view, blocks, rows
        self.send, self.own, self.near, self.far = sem
        self.s, self.c, self.hi, self.lo, self.lo1, self.lo2, self.lo3 = place

    def full(self, j):
        return self.view(j, 0, self.rows)

    def part(self, j, h):
        return self.view(j, h * (self.rows // 2), self.rows // 2)

    def direct(self, z, src=None):
        j = z * LO + self.lo
        src = self.full(j) if src is None else src
        return [
            remote(src, self.full(j), self.send.at[0], self.near.at[z], self.hi * LO + p, self.c)
            for p in (self.lo1, self.lo2)
        ]

    def diag(self, z):
        first, last = self.part(z * LO + self.lo1, 0), self.part(z * LO + self.lo2, 1)
        return [
            remote(first, first, self.send.at[0], self.far.at[z], self.hi * LO + self.lo2, self.c),
            remote(last, last, self.send.at[0], self.far.at[z], self.hi * LO + self.lo1, self.c),
        ]

    def arrived(self, ref, sem):
        remote(ref, ref, self.send.at[0], sem, self.s, 1 - self.c).wait_recv()

    def wait_own(self, z):
        self.arrived(self.full(z * LO + self.lo), self.own.at[z])

    def wait_direct(self, z):
        self.arrived(self.blocks(2), self.near.at[z])

    def wait_diag(self, z):
        self.arrived(self.full(z * LO + self.lo3), self.far.at[z])

    def wait_sent(self, planes):
        ref = self.blocks(3 * planes)
        remote(ref, ref, self.send.at[0], self.far.at[0], self.s, 1 - self.c).wait_send()


def start(copies):
    for copy in copies:
        copy.start()


def scoped(name, fn, *args):
    with jax.named_scope(name):
        return fn(*args)


def layer_kernel(HI, G, NC, names, *refs):
    r = Refs(names, refs)
    s = lax.axis_index("sp")
    c = lax.axis_index("tp")
    hi = s // LO
    lo = s % LO
    lo1 = lo + 1 - 2 * (lo % 2)
    lo2 = (lo + 2) % LO
    lo3 = (lo1 + 2) % LO
    other = 1 - c
    peers = (lo1, lo2, lo3)
    T = r.q_v.shape[0]
    H = T // 2
    D = r.tok_v.shape[1]
    R = r.up_v.shape[0]
    CH = r.up_buf.shape[1]
    W = r.dn_v.shape[1]
    PL = LO * T
    QR = 2 * PL
    own_cols = pl.ds(pl.multiple_of(hi * CH, LANES), CH)
    own_lanes = pl.ds(pl.multiple_of(lo * LANES, LANES), LANES)

    barrier = pltpu.get_barrier_semaphore()
    for p in peers:
        pl.semaphore_signal(barrier, inc=1, device_id={"sp": hi * LO + p, "tp": c}, device_id_type=MESH)
    pl.semaphore_signal(barrier, inc=1, device_id={"sp": s, "tp": other}, device_id_type=MESH)
    for dz in range(1, HI):
        far = ((hi + dz) % HI) * LO + lo
        pl.semaphore_signal(barrier, inc=1, device_id={"sp": far, "tp": c}, device_id_type=MESH)
    local = [
        (r.bias_hbm, r.bias_v),
        (r.kv_hbm, r.kv_v),
        (r.q_hbm, r.q_v),
        (r.up_hbm, r.up_v),
        (r.dn_hbm, r.dn_v),
        (r.up_hbm.at[:, own_cols], r.up_buf.at[pl.ds(s * R, R)]),
        (r.dn_hbm.at[pl.ds(hi * CH, CH)], r.dn_buf.at[s]),
        (r.tok_hbm, r.tok_v),
        (r.wo_hbm, r.wo_v),
        (r.gain_hbm, r.gain_v),
    ]
    loads = [pltpu.make_async_copy(a, b, r.load_sem.at[i]) for i, (a, b) in enumerate(local)]
    start(loads)
    loads[0].wait()

    half_lane = lax.broadcasted_iota(jnp.int32, (2 * G, LANES), 1) // HEAD
    bias = r.bias_v[...].astype(F32)
    bias = jnp.where(half_lane == lo % 2, jnp.concatenate([bias, bias], axis=1), 0.0)
    for g in range(G):
        r.bias_out[g] = bias[2 * g : 2 * g + 2]
    with jax.named_scope("barrier"):
        for load in loads[1:5]:
            load.wait()
        pl.semaphore_wait(barrier, 4 + (HI - 1))

    place = (s, c, hi, lo, lo1, lo2, lo3)
    up = Piece(
        place,
        lambda j, a, n: r.up_buf.at[pl.ds(j * R + a, n)],
        lambda n: r.up_buf.at[pl.ds(0, n * R)],
        R,
        (r.up_sp, r.up_own, r.up_near, r.up_diag),
    )
    dn = Piece(
        place,
        lambda j, a, n: r.dn_buf.at[j, pl.ds(a, n)],
        lambda n: r.dn_buf.at[pl.ds(0, n)],
        CH,
        (r.dn_sp, r.dn_own, r.dn_near, r.dn_diag),
    )

    def arrived(ref, sem):
        remote(ref, ref, r.pj_send, sem, s, other).wait_recv()

    def sent(ref, sem):
        remote(ref, ref, sem, r.pj_recv, s, other).wait_send()

    def send_keys(d, p):
        lanes = pl.ds(pl.multiple_of(p * LANES, LANES), LANES)
        dev = (hi + d) * LO + p
        return [
            remote(r.kv_v.at[:, lanes], r.kv_buf.at[hi, pl.ds(lo * T, T)], r.k_send.at[d], r.k_recv.at[hi], dev, c),
            remote(r.bias_out.at[p], r.bias_in.at[hi, lo], r.b_send.at[d], r.b_recv.at[hi], dev, c),
        ]

    def send_queries(p):
        lanes = pl.ds(pl.multiple_of(p * LANES, LANES), LANES)
        return remote(r.q_v.at[:, lanes], r.q_in.at[lo], r.q_send.at[0], r.q_recv.at[0], hi * LO + p, c)

    def keys_of(z, shards):
        arrived(r.kv_buf.at[z, pl.ds(0, shards * T)], r.k_recv.at[z])
        arrived(r.bias_in.at[z, pl.ds(0, shards)], r.b_recv.at[z])

    def join_bias(z):
        for i in range(LO // 2):
            r.bias_pl[z, :, i * LANES : (i + 1) * LANES] = r.bias_in[z, 2 * i] + r.bias_in[z, 2 * i + 1]

    def up_far(hp):
        cols = pl.ds(pl.multiple_of(hp * CH, LANES), CH)
        return remote(r.up_v.at[:, cols], up.full(s), r.wz_send.at[0], r.up_own.at[hi], hp * LO + lo, c)

    def dn_far(hp):
        rows = pl.ds(hp * CH, CH)
        return remote(r.dn_v.at[rows], dn.full(s), r.wz_send.at[1], r.dn_own.at[hi], hp * LO + lo, c)

    small = jnp.minimum(hi, HI - 1 - hi)
    tilt = jnp.where(hi <= HI - 1 - hi, 1, -1)

    def nth(k):
        if k == 0:
            return hi
        near = hi + (k + 1) // 2 if k % 2 else hi - k // 2
        return jnp.where(k <= 2 * small, near, hi + tilt * (k - small))

    def below(far, d):
        @pl.when(hi >= d)
        def _():
            far(hi - d).start()

    def above(far, d):
        @pl.when(hi + d < HI)
        def _():
            far(hi + d).start()

    for p in peers:
        pl.semaphore_signal(r.ready, inc=1, device_id={"sp": hi * LO + p, "tp": c}, device_id_type=MESH)
    for p in peers:
        start(send_keys(0, p))
        send_queries(p).start()

    def raise_keys(shards):
        for d in range(HI - 1, 0, -1):

            @pl.when(hi + d < HI)
            def _():
                for p in shards:
                    start(send_keys(d, p))

    raise_keys((lo,))
    for d in range(1, HI):
        below(up_far, d)
    scoped("ready", pl.semaphore_wait, r.ready, LO - 1)
    raise_keys(peers)
    start(up.direct(hi, r.up_v.at[:, own_cols]))
    for d in range(1, HI):
        above(up_far, d)
    start(dn.direct(hi, r.dn_v.at[pl.ds(hi * CH, CH)]))

    r.q_in[lo] = r.q_v[:, own_lanes]
    r.kv_buf[hi, pl.ds(lo * T, T), :] = r.kv_v[:, own_lanes]
    r.bias_in[hi, lo] = r.bias_out[lo]
    row_id = lax.broadcasted_iota(jnp.int32, (PL, PL + LANES), 0)
    col_id = lax.broadcasted_iota(jnp.int32, (PL, PL + LANES), 1)
    after_key = (row_id > col_id) | (col_id >= PL)
    r.tri_buf[...] = jnp.where(after_key, 1.0, 0.0).astype(BF16)
    low = lax.broadcasted_iota(jnp.int32, (T, LANES), 1) < HEAD

    with jax.named_scope("heads_wait"):
        keys_of(hi, LO - 1)
        arrived(r.q_in.at[pl.ds(0, LO - 1)], r.q_recv.at[0])
    join_bias(hi)
    for j in range(LO):
        qg = r.q_in[j].astype(F32) * 0.125
        r.q_all[j * T : (j + 1) * T] = jnp.where(low, qg, 0.0).astype(BF16)
        r.q_all[PL + j * T : PL + (j + 1) * T] = jnp.where(low, pltpu.roll(qg, HEAD, 1), 0.0).astype(BF16)

    step = 128

    def attend(z, own):
        keys = r.kv_buf[z]
        for i in range(QR // step):
            rows = slice(i * step, (i + 1) * step)
            head = i * step // PL
            scores = dot_nt(r.q_all[rows], keys) + r.bias_pl[z, head : head + 1, :]
            soft = jnp.maximum(scores, 0.0) + jnp.log(1.0 + jnp.exp(-jnp.abs(scores)))
            log_pass = -soft
            if own:
                query = i * step % PL + lax.broadcasted_iota(jnp.int32, (step, PL), 0)
                strict = lax.broadcasted_iota(jnp.int32, (step, PL), 1) < query
                log_pass = jnp.where(strict, log_pass, 0.0)
            top = log_pass.astype(BF16)
            rest = (log_pass - top.astype(F32)).astype(BF16)
            sums = jnp.dot(top, r.tri_buf[...], preferred_element_type=F32) + jnp.dot(
                rest, r.tri_buf[...], preferred_element_type=F32
            )
            power = scores - soft + sums[:, :PL]
            if not own:
                held = r.carry[rows]
                power = power + jnp.concatenate([held] * (PL // LANES), axis=1)
            weights = jnp.exp(power)
            if own:
                weights = jnp.where(strict, weights, 0.0)
            part = jnp.dot(weights.astype(BF16), keys, preferred_element_type=F32)
            if own:
                r.acc[rows] = part
                r.carry[rows] = sums[:, PL:]
            else:
                r.acc[rows] += part
                r.carry[rows] = held + sums[:, PL:]

    def look(d):
        @pl.when(hi >= d)
        def _():
            z = hi - d
            scoped(f"keys_wait{d}", keys_of, z, LO)
            join_bias(z)
            scoped(f"attend{d}", attend, z, False)

    def relay_direct(piece, k):
        scoped(f"own_wait{k}", piece.wait_own, nth(k))
        start(piece.direct(nth(k)))

    def relay_diag(piece, k):
        scoped(f"direct_wait{k}", piece.wait_direct, nth(k))
        start(piece.diag(nth(k)))

    scoped("attend0", attend, hi, True)
    relay_diag(up, 0)
    for d in range(1, HI):
        look(d)
        if d == 1:
            relay_direct(up, 1)

    heads = [r.acc[h * PL : (h + 1) * PL] for h in range(2)]
    low_pl = lax.broadcasted_iota(jnp.int32, (PL, LANES), 1) < HEAD
    r.att_pl[...] = jnp.where(low_pl, pltpu.roll(heads[0], HEAD, 1), heads[1]).astype(BF16)

    def att_back(p):
        src = r.att_pl.at[pl.ds(p * T, T)]
        return remote(src, r.att_buf.at[:, own_lanes], r.t_send.at[0], r.t_recv.at[0], hi * LO + p, c)

    for p in peers:
        att_back(p).start()
    for d in range(1, HI):
        below(dn_far, d)
        above(dn_far, d)
    relay_diag(dn, 0)
    r.att_buf[:, own_lanes] = r.att_pl[pl.ds(lo * T, T), :]
    with jax.named_scope("att_wait"):
        for load in loads[5:]:
            load.wait()
        arrived(r.att_pl.at[pl.ds(0, (LO - 1) * T)], r.t_recv.at[0])

    att = r.att_buf[...]
    wide = 512 if D % 512 == 0 else LANES
    for i in range(D // wide):
        cols = slice(i * wide, (i + 1) * wide)
        r.pj_buf[:, cols] = jnp.dot(att, r.wo_v[:, cols], preferred_element_type=F32).astype(BF16)
    pj_copy = remote(r.pj_buf.at[pl.ds(other * H, H)], r.pj_in, r.pj_send, r.pj_recv, s, other)
    pj_copy.start()
    relay_direct(up, 2)
    relay_diag(up, 1)
    scoped("pj_wait", pj_copy.wait)
    mine = pl.ds(c * H, H)
    total = r.pj_buf[mine, :].astype(F32) + r.pj_in[...].astype(F32)
    residual = (r.tok_v[mine, :].astype(F32) + total).astype(BF16)
    r.res_buf[...] = residual
    values = residual.astype(F32)
    factor = lax.rsqrt(jnp.mean(values * values, axis=-1, keepdims=True) + EPSILON)
    r.n_buf[pl.ds((c * HI + hi) * H, H), :] = (values * factor * r.gain_v[...]).astype(BF16)

    NW = D // NC

    def n_at(z, core, q):
        return r.n_buf.at[pl.ds((core * HI + z) * H, H), q * NW : (q + 1) * NW]

    def n_up(z, q):
        return remote(n_at(z, c, q), n_at(z, c, q), r.nu_send.at[z], r.nz_recv.at[z * NC + q], s + LO, c)

    def n_down(z, q):
        return remote(n_at(z, c, q), n_at(z, c, q), r.nd_send.at[z], r.nz_recv.at[z * NC + q], s - LO, c)

    def n_pass(z, q):
        return remote(n_at(z, c, q), n_at(z, c, q), r.np_send.at[0], r.nc_recv.at[0], s, other)

    for q in range(NC):

        @pl.when(hi + 1 < HI)
        def _():
            n_up(hi, q).start()

        @pl.when(hi > 0)
        def _():
            n_down(hi, q).start()

    for q in range(NC):
        n_pass(hi, q).start()

    upper = hi // (HI // 2)

    def norm_take(k):
        rank = hi + upper * (HI - 1 - 2 * hi)
        z = k - 1 + (rank < k).astype(jnp.int32)
        z = z + upper * (HI - 1 - 2 * z)
        for q in range(NC):
            scoped(f"norm_wait{k}", arrived, n_at(z, c, q), r.nz_recv.at[z * NC + q])

            @pl.when((z < hi) & (hi + 1 < HI))
            def _():
                n_up(z, q).start()

            @pl.when((z > hi) & (hi > 0))
            def _():
                n_down(z, q).start()

            n_pass(z, q).start()

    for k in range(3, HI):
        relay_direct(up, k)
        relay_diag(up, k - 1)
    relay_direct(dn, 1)
    for k in range(1, HI):
        norm_take(k)
        if k == 1:
            relay_diag(up, HI - 1)
        else:
            relay_diag(dn, k - 1)
        if k + 1 < HI:
            relay_direct(dn, k + 1)
    with jax.named_scope("norm_other_wait"):
        arrived(r.n_buf.at[pl.ds(0, HI * H)], r.nc_recv.at[0])
    with jax.named_scope("up_wait"):
        for k in range(HI):
            up.wait_diag(nth(k))

    wide = 256 if CH % 256 == 0 else LANES
    for i in range(CH // wide):
        cols = slice(i * wide, (i + 1) * wide)
        raw = jnp.maximum(jnp.dot(r.n_buf[...], r.up_buf[:, cols], preferred_element_type=F32), 0.0)
        r.hid_buf[:, cols] = (raw * raw).astype(BF16)
    half = HI * H
    CW = LO * W
    mine_rows = pl.ds(c * half, half)

    def x_out(k):
        z = nth(k)
        rows = pl.ds(other * half, half)
        return remote(r.ps_buf.at[z, rows], r.x_in.at[z], r.x_send.at[0], r.x_recv.at[z], s, other)

    def p_out(z, far):
        hp = (hi + far) % HI
        return remote(r.xs_buf.at[z, pl.ds(hp * H, H)], r.pr_buf.at[z, hi], r.p_send.at[0], r.p_recv.at[z], hp * LO + lo, c)

    def spread(k):
        z = nth(k)
        scoped(f"x_wait{k}", arrived, r.x_in.at[z], r.x_recv.at[z])
        mixed = r.ps_buf[z, mine_rows, :].astype(F32) + r.x_in[z].astype(F32)
        r.xs_buf[z] = mixed.astype(BF16)

        for far in range(1, HI):
            p_out(z, far).start()

    relay_diag(dn, HI - 1)
    for k in range(HI):
        z = nth(k)
        scoped(f"dn_wait{k}", dn.wait_diag, z)
        for q in range(0, LO, 2):
            pair = jnp.concatenate([r.dn_buf[z * LO + q], r.dn_buf[z * LO + q + 1]], axis=1)
            part = jnp.dot(r.hid_buf[...], pair, preferred_element_type=F32)
            r.ps_buf[z, :, q * W : (q + 2) * W] = part.astype(BF16)
        x_out(k).start()
        if k > 0:
            spread(k - 1)
    spread(HI - 1)

    def drain():
        for z in range(1, HI):

            @pl.when(hi + z < HI)
            def _():
                sent(r.kv_buf.at[0], r.k_send.at[z])
                sent(r.bias_in.at[0], r.b_send.at[z])

        sent(r.kv_buf.at[0, pl.ds(0, (LO - 1) * T)], r.k_send.at[0])
        sent(r.bias_in.at[0, pl.ds(0, LO - 1)], r.b_send.at[0])
        sent(r.q_in.at[pl.ds(0, LO - 1)], r.q_send.at[0])
        sent(r.att_pl.at[pl.ds(0, (LO - 1) * T)], r.t_send.at[0])
        sent(up.blocks(HI - 1), r.wz_send.at[0])
        sent(dn.blocks(HI - 1), r.wz_send.at[1])
        up.wait_sent(HI)
        dn.wait_sent(HI)
        for z in range(HI):

            @pl.when((z <= hi) & (hi + 1 < HI))
            def _():
                sent(r.res_buf, r.nu_send.at[z])

            @pl.when((z >= hi) & (hi > 0))
            def _():
                sent(r.res_buf, r.nd_send.at[z])

        sent(r.n_buf.at[pl.ds(0, HI * H)], r.np_send.at[0])
        sent(r.x_in, r.x_send.at[0])

    scoped("drain", drain)
    for k in range(HI):
        z = nth(k)
        cols = pl.ds(pl.multiple_of(z * CW, LANES), CW)
        update = r.xs_buf[z, pl.ds(hi * H, H), :].astype(F32)
        scoped(f"sum_wait{k}", arrived, r.pr_buf.at[z, pl.ds(0, HI - 1)], r.p_recv.at[z])
        for far in range(1, HI):
            update = update + r.pr_buf[z, (hi + far) % HI].astype(F32)
        r.out_ref[:, cols] = (r.res_buf[:, cols].astype(F32) + update).astype(BF16)
    sent(r.pr_buf.at[:, pl.ds(0, HI - 1)], r.p_send.at[0])


def fits(tokens, queries, key_values, stop_bias, up_proj, down_proj):
    sp = lax.axis_size("sp")
    rows, seqs, heads = stop_bias.shape
    hidden = up_proj.shape[1]
    return (
        lax.axis_size("tp") == 2
        and sp == LO * LO
        and seqs == 1
        and heads == 2 * LO
        and queries.shape[2] == heads * HEAD
        and key_values.shape[2] == heads * HEAD
        and 2 * HEAD == LANES
        and 2 * rows == LANES
        and hidden % (sp // LO * LANES) == 0
        and down_proj.shape[1] % LANES == 0
        and up_proj.shape[0] % 16 == 0
        and tokens.shape[2] % 512 == 0
    )


def body(tokens, queries, key_values, stop_bias, out_proj, norm_gain, up_proj, down_proj):
    if not fits(tokens, queries, key_values, stop_bias, up_proj, down_proj):
        return general_body(
            tokens, queries, key_values, stop_bias, out_proj, norm_gain, up_proj, down_proj
        )
    sp = lax.axis_size("sp")
    HI = sp // LO
    T, _, D = tokens.shape
    H = T // 2
    heads = stop_bias.shape[2]
    G = heads // 2
    R, hidden = up_proj.shape
    CH = hidden // HI
    W = down_proj.shape[1]
    PL = LO * T
    NC = 4
    vmem = pl.BlockSpec(memory_space=pltpu.VMEM)
    hbm = pl.BlockSpec(memory_space=pl.ANY)

    def sem(*shape):
        return pltpu.SemaphoreType.DMA(shape)

    operands = dict(
        tok_hbm=(tokens.reshape(T, D), hbm),
        q_hbm=(queries.reshape(T, queries.shape[2]), hbm),
        kv_hbm=(key_values.reshape(T, key_values.shape[2]), hbm),
        bias_hbm=(stop_bias.reshape(T, heads).T, hbm),
        wo_hbm=(out_proj, hbm),
        gain_hbm=(norm_gain.reshape(1, D), hbm),
        up_hbm=(up_proj, hbm),
        dn_hbm=(down_proj, hbm),
    )
    scratch = dict(
        tok_v=pltpu.VMEM((T, D), BF16),
        bias_v=pltpu.VMEM((heads, T), BF16),
        q_v=pltpu.VMEM((T, G * LANES), BF16),
        kv_v=pltpu.VMEM((T, G * LANES), BF16),
        wo_v=pltpu.VMEM(out_proj.shape, BF16),
        gain_v=pltpu.VMEM((1, D), F32),
        up_v=pltpu.VMEM((R, hidden), BF16),
        dn_v=pltpu.VMEM((hidden, W), BF16),
        up_buf=pltpu.VMEM((sp * R, CH), BF16),
        dn_buf=pltpu.VMEM((sp, CH, W), BF16),
        bias_out=pltpu.VMEM((G, 2, LANES), F32),
        bias_in=pltpu.VMEM((HI, LO, 2, LANES), F32),
        bias_pl=pltpu.VMEM((HI, 2, PL), F32),
        q_in=pltpu.VMEM((LO, T, LANES), BF16),
        q_all=pltpu.VMEM((2 * PL, LANES), BF16),
        kv_buf=pltpu.VMEM((HI, PL, LANES), BF16),
        tri_buf=pltpu.VMEM((PL, PL + LANES), BF16),
        carry=pltpu.VMEM((2 * PL, LANES), F32),
        acc=pltpu.VMEM((2 * PL, LANES), F32),
        att_pl=pltpu.VMEM((PL, LANES), BF16),
        att_buf=pltpu.VMEM((T, G * LANES), BF16),
        pj_buf=pltpu.VMEM((T, D), BF16),
        pj_in=pltpu.VMEM((H, D), BF16),
        res_buf=pltpu.VMEM((H, D), BF16),
        n_buf=pltpu.VMEM((HI * T, D), BF16),
        hid_buf=pltpu.VMEM((HI * T, CH), BF16),
        ps_buf=pltpu.VMEM((HI, HI * T, LO * W), BF16),
        x_in=pltpu.VMEM((HI, HI * H, LO * W), BF16),
        xs_buf=pltpu.VMEM((HI, HI * H, LO * W), BF16),
        pr_buf=pltpu.VMEM((HI, HI, H, LO * W), BF16),
        load_sem=sem(10),
        k_send=sem(HI),
        b_send=sem(HI),
        ready=pltpu.SemaphoreType.REGULAR,
        q_send=sem(1),
        k_recv=sem(HI),
        b_recv=sem(HI),
        q_recv=sem(1),
        wz_send=sem(2),
        up_sp=sem(1),
        up_own=sem(HI),
        up_near=sem(HI),
        up_diag=sem(HI),
        dn_sp=sem(1),
        dn_own=sem(HI),
        dn_near=sem(HI),
        dn_diag=sem(HI),
        t_send=sem(1),
        t_recv=sem(1),
        pj_send=pltpu.SemaphoreType.DMA,
        pj_recv=pltpu.SemaphoreType.DMA,
        nu_send=sem(HI),
        nd_send=sem(HI),
        np_send=sem(1),
        nz_recv=sem(HI * NC),
        nc_recv=sem(1),
        x_send=sem(1),
        x_recv=sem(HI),
        p_send=sem(1),
        p_recv=sem(HI),
    )
    names = [*operands, "out_ref", *scratch]
    out = pl.pallas_call(
        lambda *refs: layer_kernel(HI, G, NC, names, *refs),
        out_shape=pltpu.VMEM((H, D), BF16),
        in_specs=[spec for _, spec in operands.values()],
        out_specs=vmem,
        scratch_shapes=list(scratch.values()),
        compiler_params=pltpu.CompilerParams(
            collective_id=0, has_side_effects=True, vmem_limit_bytes=56 * 1024 * 1024
        ),
        name="layer",
    )(*[value for value, _ in operands.values()])
    return out.reshape(H, 1, D)


def solution(mesh):
    return jax.shard_map(
        body,
        mesh=mesh,
        in_specs=(
            P("sp", None, None),
            P("sp", None, "tp"),
            P("sp", None, "tp"),
            P("sp", None, "tp"),
            P("tp", None),
            P(),
            P("sp", "tp"),
            P("tp", "sp"),
        ),
        out_specs=P(("sp", "tp"), None, None),
        check_vma=False,
    )
```

```python
import math

import jax
import jax.numpy as jnp
from jax import lax
from jax.experimental import pallas as pl
from jax.experimental.pallas import tpu as pltpu
from jax.sharding import PartitionSpec as P

HEAD = 64


EPSILON = 1e-06


def rms_scale(residual, gain):
    values = residual.astype(jnp.float32)
    factor = lax.rsqrt(jnp.mean(values * values, axis=-1, keepdims=True) + EPSILON)
    return (values * factor * gain).astype(jnp.bfloat16)


def sweep_keys(totals, pieces, shard_rows, step_fn):
    kv_rows, bias_rows = pieces
    shards = kv_rows.shape[0] // shard_rows
    group_shards = math.gcd(shards, max(1, 1024 // shard_rows))
    span_rows = group_shards * shard_rows

    def advance(number, running):
        first_row = number * span_rows
        kv_block = lax.dynamic_slice_in_dim(kv_rows, first_row, span_rows, 0)
        bias_block = lax.dynamic_slice_in_dim(bias_rows, first_row, span_rows, 0)
        return step_fn(running, kv_block, bias_block, first_row, group_shards)

    return lax.fori_loop(0, shards // group_shards, advance, totals)


def general_body(tokens, queries, key_values, stop_bias, out_proj, norm_gain, up_proj, down_proj):
    row_count = tokens.shape[0]
    seq_count = tokens.shape[1]
    head_count = queries.shape[2] // HEAD
    kv_count = key_values.shape[2] // (2 * HEAD)
    group_size = head_count // kv_count
    n_shards = lax.axis_size("sp")
    query_start = lax.axis_index("sp") * row_count
    query_pos = query_start + lax.iota(jnp.int32, row_count)
    q_heads = queries.reshape(row_count, seq_count, kv_count, group_size, HEAD).transpose(
        1, 2, 3, 0, 4
    )
    q_heads = q_heads.reshape(seq_count, kv_count, group_size * row_count, HEAD)

    def stick_block(kv_block, bias_block, key_start):
        span_rows = kv_block.shape[0]
        key_pairs = kv_block.reshape(span_rows, seq_count, kv_count, 2 * HEAD)
        keys_part = key_pairs[..., :HEAD]
        values_part = key_pairs[..., HEAD:]
        scores = (
            jnp.einsum("bgmd,sbgd->bgms", q_heads, keys_part, preferred_element_type=jnp.float32)
            * 0.125
        )
        bias_float = jnp.transpose(bias_block, (1, 2, 0)).astype(jnp.float32)
        scores = (
            scores.reshape(seq_count, head_count, row_count, span_rows) + bias_float[:, :, None, :]
        )
        key_pos = key_start + lax.iota(jnp.int32, span_rows)
        strict = key_pos[None, :] < query_pos[:, None]
        log_pass = jnp.where(strict, jax.nn.log_sigmoid(-scores), 0.0)
        return (scores, strict, log_pass, values_part)

    def weigh(scores, strict, after_sum, values_part):
        span_rows = scores.shape[3]
        weights = jnp.where(strict, jnp.exp(jax.nn.log_sigmoid(scores) + after_sum), 0.0).astype(
            jnp.bfloat16
        )
        weights = weights.reshape(seq_count, kv_count, group_size * row_count, span_rows)
        return jnp.einsum(
            "bgms,sbgd->bgmd", weights, values_part, preferred_element_type=jnp.float32
        )

    empty_out = jnp.zeros((seq_count, kv_count, group_size * row_count, HEAD), jnp.float32)

    def sum_step(sums_table, kv_block, bias_block, key_start, shard_group):

        def sum_compute(table_in):
            scores, strict, log_pass, values_part = stick_block(kv_block, bias_block, key_start)
            block_sums = log_pass.reshape(
                seq_count, head_count, row_count, shard_group, row_count
            ).sum(axis=4)
            slot_index = key_start // row_count
            current = lax.dynamic_slice_in_dim(table_in, slot_index, shard_group, 0)
            return lax.dynamic_update_slice_in_dim(
                table_in, current + jnp.transpose(block_sums, (3, 0, 1, 2)), slot_index, 0
            )

        return lax.cond(
            key_start < query_start + row_count, sum_compute, lambda table_in: table_in, sums_table
        )

    empty_table = jnp.zeros((n_shards, seq_count, head_count, row_count), jnp.float32)
    sums_table = sweep_keys(
        empty_table,
        (
            lax.all_gather(key_values, "sp", axis=0, tiled=True),
            lax.all_gather(stop_bias, "sp", axis=0, tiled=True),
        ),
        row_count,
        sum_step,
    )
    offsets = lax.cumsum(sums_table, axis=0, reverse=True) - sums_table

    def out_step(outputs, kv_block, bias_block, key_start, shard_group):

        def out_compute(running):
            scores, strict, log_pass, values_part = stick_block(kv_block, bias_block, key_start)
            span_rows = kv_block.shape[0]
            split_pass = log_pass.reshape(seq_count, head_count, row_count, shard_group, row_count)
            within = lax.cumsum(split_pass, axis=4, reverse=True) - split_pass
            carried = lax.dynamic_slice_in_dim(offsets, key_start // row_count, shard_group, 0)
            carried = jnp.transpose(carried, (1, 2, 3, 0))[..., None]
            after_sum = (within + carried).reshape(seq_count, head_count, row_count, span_rows)
            return running + weigh(scores, strict, after_sum, values_part)

        return lax.cond(
            key_start < query_start + row_count, out_compute, lambda running: running, outputs
        )

    accum_out = sweep_keys(
        empty_out,
        (
            lax.all_gather(key_values, "sp", axis=0, tiled=True),
            lax.all_gather(stop_bias, "sp", axis=0, tiled=True),
        ),
        row_count,
        out_step,
    )
    attended = accum_out.reshape(seq_count, kv_count, group_size, row_count, HEAD).transpose(
        3, 0, 1, 2, 4
    )
    attended = attended.reshape(row_count * seq_count, head_count * HEAD).astype(jnp.bfloat16)
    share_tokens = row_count // lax.axis_size("tp")
    share_rows = share_tokens * seq_count
    tp_index = lax.axis_index("tp")
    projected = lax.psum(
        jnp.dot(attended, out_proj, preferred_element_type=jnp.float32).astype(jnp.bfloat16), "tp"
    ).astype(jnp.float32)
    flat_tokens = tokens.reshape(row_count * seq_count, tokens.shape[2])
    residual = (flat_tokens.astype(jnp.float32) + projected).astype(jnp.bfloat16)
    normed = rms_scale(residual, norm_gain)
    residual_share = lax.dynamic_slice_in_dim(residual, tp_index * share_rows, share_rows, 0)
    up_values = jnp.dot(
        normed,
        lax.all_gather(up_proj, "sp", axis=0, tiled=True),
        preferred_element_type=jnp.float32,
    )
    hidden = jnp.square(jax.nn.relu(up_values)).astype(jnp.bfloat16)
    partial_terms = jnp.dot(
        hidden,
        lax.all_gather(down_proj, "sp", axis=1, tiled=True),
        preferred_element_type=jnp.float32,
    )
    update = lax.psum_scatter(
        partial_terms.astype(jnp.bfloat16), "tp", scatter_dimension=0, tiled=True
    ).astype(jnp.float32)
    result = (residual_share.astype(jnp.float32) + update).astype(jnp.bfloat16)
    return result.reshape(share_tokens, seq_count, result.shape[1])


MESH = pl.DeviceIdType.MESH
LO = 4
LANES = 128
F32 = jnp.float32
BF16 = jnp.bfloat16


def remote(src, dst, send, recv, sp, tp):
    return pltpu.make_async_remote_copy(
        src_ref=src,
        dst_ref=dst,
        send_sem=send,
        recv_sem=recv,
        device_id={"sp": sp, "tp": tp},
        device_id_type=MESH,
    )


def dot_nt(a, b):
    return lax.dot_general(a, b, (((1,), (1,)), ((), ())), preferred_element_type=F32)


def dot_tn(a, b):
    return lax.dot_general(a, b, (((0,), (0,)), ((), ())), preferred_element_type=F32)


class Refs:
    def __init__(self, names, refs):
        for name, ref in zip(names, refs):
            setattr(self, name, ref)


class Piece:
    def __init__(self, place, view, blocks, rows, sem):
        self.view, self.blocks, self.rows = view, blocks, rows
        self.send, self.own, self.near, self.far = sem
        self.s, self.c, self.hi, self.lo, self.lo1, self.lo2, self.lo3 = place

    def full(self, j):
        return self.view(j, 0, self.rows)

    def part(self, j, h):
        return self.view(j, h * (self.rows // 2), self.rows // 2)

    def direct(self, z, src=None):
        j = z * LO + self.lo
        src = self.full(j) if src is None else src
        return [
            remote(src, self.full(j), self.send.at[0], self.near.at[z], self.hi * LO + p, self.c)
            for p in (self.lo1, self.lo2)
        ]

    def diag(self, z):
        first, last = self.part(z * LO + self.lo1, 0), self.part(z * LO + self.lo2, 1)
        return [
            remote(first, first, self.send.at[0], self.far.at[z], self.hi * LO + self.lo2, self.c),
            remote(last, last, self.send.at[0], self.far.at[z], self.hi * LO + self.lo1, self.c),
        ]

    def arrived(self, ref, sem):
        remote(ref, ref, self.send.at[0], sem, self.s, 1 - self.c).wait_recv()

    def wait_own(self, z):
        self.arrived(self.full(z * LO + self.lo), self.own.at[z])

    def wait_direct(self, z):
        self.arrived(self.blocks(2), self.near.at[z])

    def wait_diag(self, z):
        self.arrived(self.full(z * LO + self.lo3), self.far.at[z])

    def wait_sent(self, planes):
        ref = self.blocks(3 * planes)
        remote(ref, ref, self.send.at[0], self.far.at[0], self.s, 1 - self.c).wait_send()


def start(copies):
    for copy in copies:
        copy.start()


def scoped(name, fn, *args):
    with jax.named_scope(name):
        return fn(*args)


def layer_kernel(HI, G, NC, names, *refs):
    r = Refs(names, refs)
    s = lax.axis_index("sp")
    c = lax.axis_index("tp")
    hi = s // LO
    lo = s % LO
    lo1 = lo + 1 - 2 * (lo % 2)
    lo2 = (lo + 2) % LO
    lo3 = (lo1 + 2) % LO
    other = 1 - c
    peers = (lo1, lo2, lo3)
    T = r.q_v.shape[0]
    H = T // 2
    D = r.tok_v.shape[1]
    R = r.up_v.shape[0]
    CH = r.up_buf.shape[1]
    W = r.dn_v.shape[1]
    PL = LO * T
    QR = 2 * PL
    own_cols = pl.ds(pl.multiple_of(hi * CH, LANES), CH)
    own_lanes = pl.ds(pl.multiple_of(lo * LANES, LANES), LANES)

    barrier = pltpu.get_barrier_semaphore()
    for p in peers:
        pl.semaphore_signal(barrier, inc=1, device_id={"sp": hi * LO + p, "tp": c}, device_id_type=MESH)
    pl.semaphore_signal(barrier, inc=1, device_id={"sp": s, "tp": other}, device_id_type=MESH)
    for dz in range(1, HI):
        far = ((hi + dz) % HI) * LO + lo
        pl.semaphore_signal(barrier, inc=1, device_id={"sp": far, "tp": c}, device_id_type=MESH)
    local = [
        (r.bias_hbm, r.bias_v),
        (r.kv_hbm, r.kv_v),
        (r.q_hbm, r.q_v),
        (r.up_hbm, r.up_v),
        (r.dn_hbm, r.dn_v),
        (r.up_hbm.at[:, own_cols], r.up_buf.at[pl.ds(s * R, R)]),
        (r.dn_hbm.at[pl.ds(hi * CH, CH)], r.dn_buf.at[s]),
        (r.tok_hbm, r.tok_v),
        (r.wo_hbm, r.wo_v),
        (r.gain_hbm, r.gain_v),
    ]
    loads = [pltpu.make_async_copy(a, b, r.load_sem.at[i]) for i, (a, b) in enumerate(local)]
    start(loads)
    loads[0].wait()

    half_lane = lax.broadcasted_iota(jnp.int32, (2 * G, LANES), 1) // HEAD
    bias = r.bias_v[...].astype(F32)
    bias = jnp.where(half_lane == lo % 2, jnp.concatenate([bias, bias], axis=1), 0.0)
    for g in range(G):
        r.bias_out[g] = bias[2 * g : 2 * g + 2]
    with jax.named_scope("barrier"):
        for load in loads[1:5]:
            load.wait()
        pl.semaphore_wait(barrier, 4 + (HI - 1))

    place = (s, c, hi, lo, lo1, lo2, lo3)
    up = Piece(
        place,
        lambda j, a, n: r.up_buf.at[pl.ds(j * R + a, n)],
        lambda n: r.up_buf.at[pl.ds(0, n * R)],
        R,
        (r.up_sp, r.up_own, r.up_near, r.up_diag),
    )
    dn = Piece(
        place,
        lambda j, a, n: r.dn_buf.at[j, pl.ds(a, n)],
        lambda n: r.dn_buf.at[pl.ds(0, n)],
        CH,
        (r.dn_sp, r.dn_own, r.dn_near, r.dn_diag),
    )

    def arrived(ref, sem):
        remote(ref, ref, r.pj_send, sem, s, other).wait_recv()

    def sent(ref, sem):
        remote(ref, ref, sem, r.pj_recv, s, other).wait_send()

    def send_keys(d, p):
        lanes = pl.ds(pl.multiple_of(p * LANES, LANES), LANES)
        dev = (hi + d) * LO + p
        return [
            remote(r.kv_v.at[:, lanes], r.kv_buf.at[hi, pl.ds(lo * T, T)], r.k_send.at[d], r.k_recv.at[hi], dev, c),
            remote(r.bias_out.at[p], r.bias_in.at[hi, lo], r.b_send.at[d], r.b_recv.at[hi], dev, c),
        ]

    def send_queries(p):
        lanes = pl.ds(pl.multiple_of(p * LANES, LANES), LANES)
        return remote(r.q_v.at[:, lanes], r.q_in.at[lo], r.q_send.at[0], r.q_recv.at[0], hi * LO + p, c)

    def keys_of(z, shards):
        arrived(r.kv_buf.at[z, pl.ds(0, shards * T)], r.k_recv.at[z])
        arrived(r.bias_in.at[z, pl.ds(0, shards)], r.b_recv.at[z])

    def join_bias(z):
        for i in range(LO // 2):
            r.bias_pl[z, :, i * LANES : (i + 1) * LANES] = r.bias_in[z, 2 * i] + r.bias_in[z, 2 * i + 1]

    def up_far(hp):
        cols = pl.ds(pl.multiple_of(hp * CH, LANES), CH)
        return remote(r.up_v.at[:, cols], up.full(s), r.wz_send.at[0], r.up_own.at[hi], hp * LO + lo, c)

    def dn_far(hp):
        rows = pl.ds(hp * CH, CH)
        return remote(r.dn_v.at[rows], dn.full(s), r.wz_send.at[1], r.dn_own.at[hi], hp * LO + lo, c)

    small = jnp.minimum(hi, HI - 1 - hi)
    tilt = jnp.where(hi <= HI - 1 - hi, 1, -1)

    def nth(k):
        if k == 0:
            return hi
        near = hi + (k + 1) // 2 if k % 2 else hi - k // 2
        return jnp.where(k <= 2 * small, near, hi + tilt * (k - small))

    upper = hi // (HI // 2)
    rank = hi + upper * (HI - 1 - 2 * hi)

    def order(k):
        if k == 0:
            return hi
        z = k - 1 + (rank < k).astype(jnp.int32)
        return z + upper * (HI - 1 - 2 * z)

    def below(far, d):
        @pl.when(hi >= d)
        def _():
            far(hi - d).start()

    def above(far, d):
        @pl.when(hi + d < HI)
        def _():
            far(hi + d).start()

    for p in peers:
        pl.semaphore_signal(r.ready, inc=1, device_id={"sp": hi * LO + p, "tp": c}, device_id_type=MESH)
    for p in peers:
        start(send_keys(0, p))
        send_queries(p).start()

    def raise_keys(shards):
        for d in range(HI - 1, 0, -1):

            @pl.when(hi + d < HI)
            def _():
                for p in shards:
                    start(send_keys(d, p))

    raise_keys((lo,))
    pair = hi + 1 - 2 * (hi % 2)
    for d in range(1, HI):
        below(up_far, d)
        if d == 1:
            pl.when(hi % 2 == 1)(lambda: dn_far(pair).start())
    scoped("ready", pl.semaphore_wait, r.ready, LO - 1)
    raise_keys(peers)
    start(up.direct(hi, r.up_v.at[:, own_cols]))
    for d in range(1, HI):
        above(up_far, d)
        if d == 1:
            pl.when(hi % 2 == 0)(lambda: dn_far(pair).start())
    start(dn.direct(hi, r.dn_v.at[pl.ds(hi * CH, CH)]))

    r.q_in[lo] = r.q_v[:, own_lanes]
    r.kv_buf[hi, pl.ds(lo * T, T), :] = r.kv_v[:, own_lanes]
    r.bias_in[hi, lo] = r.bias_out[lo]
    row_id = lax.broadcasted_iota(jnp.int32, (PL, PL + LANES), 0)
    col_id = lax.broadcasted_iota(jnp.int32, (PL, PL + LANES), 1)
    after_key = (row_id > col_id) | (col_id >= PL)
    r.tri_buf[...] = jnp.where(after_key, 1.0, 0.0).astype(BF16)
    low = lax.broadcasted_iota(jnp.int32, (T, LANES), 1) < HEAD

    with jax.named_scope("heads_wait"):
        keys_of(hi, LO - 1)
        arrived(r.q_in.at[pl.ds(0, LO - 1)], r.q_recv.at[0])
    join_bias(hi)
    for j in range(LO):
        qg = r.q_in[j].astype(F32) * 0.125
        r.q_all[j * T : (j + 1) * T] = jnp.where(low, qg, 0.0).astype(BF16)
        r.q_all[PL + j * T : PL + (j + 1) * T] = jnp.where(low, pltpu.roll(qg, HEAD, 1), 0.0).astype(BF16)

    step = 128

    def attend(z, own):
        keys = r.kv_buf[z]
        for i in range(QR // step):
            rows = slice(i * step, (i + 1) * step)
            head = i * step // PL
            scores = dot_nt(r.q_all[rows], keys) + r.bias_pl[z, head : head + 1, :]
            soft = jnp.maximum(scores, 0.0) + jnp.log(1.0 + jnp.exp(-jnp.abs(scores)))
            log_pass = -soft
            if own:
                query = i * step % PL + lax.broadcasted_iota(jnp.int32, (step, PL), 0)
                strict = lax.broadcasted_iota(jnp.int32, (step, PL), 1) < query
                log_pass = jnp.where(strict, log_pass, 0.0)
            top = log_pass.astype(BF16)
            rest = (log_pass - top.astype(F32)).astype(BF16)
            sums = jnp.dot(top, r.tri_buf[...], preferred_element_type=F32) + jnp.dot(
                rest, r.tri_buf[...], preferred_element_type=F32
            )
            power = scores - soft + sums[:, :PL]
            if not own:
                held = r.carry[rows]
                power = power + jnp.concatenate([held] * (PL // LANES), axis=1)
            weights = jnp.exp(power)
            if own:
                weights = jnp.where(strict, weights, 0.0)
            part = jnp.dot(weights.astype(BF16), keys, preferred_element_type=F32)
            if own:
                r.acc[rows] = part
                r.carry[rows] = sums[:, PL:]
            else:
                r.acc[rows] += part
                r.carry[rows] = held + sums[:, PL:]

    def look(d):
        @pl.when(hi >= d)
        def _():
            z = hi - d
            scoped(f"keys_wait{d}", keys_of, z, LO)
            join_bias(z)
            scoped(f"attend{d}", attend, z, False)

    def relay_direct(piece, k):
        z = nth(k) if piece is up else order(k)
        scoped(f"{'UD'[piece is dn]}own_wait{k}", piece.wait_own, z)
        start(piece.direct(z))

    def relay_diag(piece, k):
        z = nth(k) if piece is up else order(k)
        scoped(f"{'UD'[piece is dn]}direct_wait{k}", piece.wait_direct, z)
        start(piece.diag(z))

    scoped("attend0", attend, hi, True)
    relay_diag(up, 0)
    for d in range(1, HI):
        look(d)
        if d == 1:
            relay_direct(up, 1)

    heads = [r.acc[h * PL : (h + 1) * PL] for h in range(2)]
    low_pl = lax.broadcasted_iota(jnp.int32, (PL, LANES), 1) < HEAD
    r.att_pl[...] = jnp.where(low_pl, pltpu.roll(heads[0], HEAD, 1), heads[1]).astype(BF16)

    def att_back(p):
        src = r.att_pl.at[pl.ds(p * T, T)]
        return remote(src, r.att_buf.at[:, own_lanes], r.t_send.at[0], r.t_recv.at[0], hi * LO + p, c)

    for p in peers:
        att_back(p).start()

    def dn_rest():
        for d in range(1, HI):

            @pl.when((hi >= d) & (hi - d != pair))
            def _():
                dn_far(hi - d).start()

            @pl.when((hi + d < HI) & (hi + d != pair))
            def _():
                dn_far(hi + d).start()

    r.att_buf[:, own_lanes] = r.att_pl[pl.ds(lo * T, T), :]
    relay_diag(dn, 0)
    pl.when(upper == 0)(lambda: relay_direct(up, 2))
    with jax.named_scope("att_wait"):
        for load in loads[5:]:
            load.wait()
        arrived(r.att_pl.at[pl.ds(0, (LO - 1) * T)], r.t_recv.at[0])

    att = r.att_buf[...]
    wide = 512 if D % 512 == 0 else LANES
    for i in range(D // wide):
        cols = slice(i * wide, (i + 1) * wide)
        r.pj_buf[:, cols] = jnp.dot(att, r.wo_v[:, cols], preferred_element_type=F32).astype(BF16)
    pj_copy = remote(r.pj_buf.at[pl.ds(other * H, H)], r.pj_in, r.pj_send, r.pj_recv, s, other)
    pj_copy.start()
    dn_rest()
    relay_diag(up, 1)
    relay_direct(dn, 1)
    pl.when(upper == 1)(lambda: relay_direct(up, 2))
    scoped("pj_wait", pj_copy.wait)
    mine = pl.ds(c * H, H)
    total = r.pj_buf[mine, :].astype(F32) + r.pj_in[...].astype(F32)
    residual = (r.tok_v[mine, :].astype(F32) + total).astype(BF16)
    r.res_buf[...] = residual
    values = residual.astype(F32)
    factor = lax.rsqrt(jnp.mean(values * values, axis=-1, keepdims=True) + EPSILON)
    r.n_buf[pl.ds((c * HI + hi) * H, H), :] = (values * factor * r.gain_v[...]).astype(BF16)

    NW = D // NC

    def n_at(z, core, q):
        return r.n_buf.at[pl.ds((core * HI + z) * H, H), q * NW : (q + 1) * NW]

    def n_up(z, q):
        return remote(n_at(z, c, q), n_at(z, c, q), r.nu_send.at[z], r.nz_recv.at[z * NC + q], s + LO, c)

    def n_down(z, q):
        return remote(n_at(z, c, q), n_at(z, c, q), r.nd_send.at[z], r.nz_recv.at[z * NC + q], s - LO, c)

    def n_pass(z, q):
        return remote(n_at(z, c, q), n_at(z, c, q), r.np_send.at[0], r.nc_recv.at[0], s, other)

    for q in range(NC):

        @pl.when(hi + 1 < HI)
        def _():
            n_up(hi, q).start()

        @pl.when(hi > 0)
        def _():
            n_down(hi, q).start()

    for q in range(NC):
        n_pass(hi, q).start()

    def norm_take(k):
        z = order(k)
        for q in range(NC):
            scoped(f"norm_wait{k}", arrived, n_at(z, c, q), r.nz_recv.at[z * NC + q])

            @pl.when((z < hi) & (hi + 1 < HI))
            def _():
                n_up(z, q).start()

            @pl.when((z > hi) & (hi > 0))
            def _():
                n_down(z, q).start()

            n_pass(z, q).start()

    relay_direct(up, 3)
    relay_diag(up, 2)
    relay_diag(dn, 1)
    norm_take(1)
    relay_diag(up, 3)
    relay_direct(dn, 2)
    norm_take(2)
    relay_direct(dn, 3)
    norm_take(3)
    relay_diag(dn, 2)
    with jax.named_scope("norm_other_wait"):
        arrived(r.n_buf.at[pl.ds(0, HI * H)], r.nc_recv.at[0])
    with jax.named_scope("up_wait"):
        for k in range(HI):
            up.wait_diag(nth(k))

    wide = 256 if CH % 256 == 0 else LANES
    for i in range(CH // wide):
        cols = slice(i * wide, (i + 1) * wide)
        raw = jnp.maximum(jnp.dot(r.n_buf[...], r.up_buf[:, cols], preferred_element_type=F32), 0.0)
        r.hid_buf[:, cols] = (raw * raw).astype(BF16)
    half = HI * H
    CW = LO * W
    mine_rows = pl.ds(c * half, half)

    def x_out(k):
        z = order(k)
        rows = pl.ds(other * half, half)
        return remote(r.ps_buf.at[z, rows], r.x_in.at[z], r.x_send.at[0], r.x_recv.at[z], s, other)

    edge = (hi == 0) | (hi == HI - 1)
    near = hi + 1 - 2 * (hi % 2)
    away = (1 - upper) * (HI - 1)
    middle = away + 2 * upper - 1

    def p_out(z, hp):
        return remote(r.xs_buf.at[z, pl.ds(hp * H, H)], r.pr_buf.at[z, hi], r.p_send.at[0], r.p_recv.at[z], hp * LO + lo, c)

    def spread(k):
        z = order(k)
        scoped(f"x_wait{k}", arrived, r.x_in.at[z], r.x_recv.at[z])
        mixed = r.ps_buf[z, mine_rows, :].astype(F32) + r.x_in[z].astype(F32)
        r.xs_buf[z] = mixed.astype(BF16)

        p_out(z, away).start()
        p_out(z, middle).start()
        pl.when(jnp.logical_not(edge))(lambda: p_out(z, near).start())

    for k in range(HI):
        z = order(k)
        scoped(f"dn_wait{k}", dn.wait_diag, z)
        for q in range(0, LO, 2):
            pair = jnp.concatenate([r.dn_buf[z * LO + q], r.dn_buf[z * LO + q + 1]], axis=1)
            part = jnp.dot(r.hid_buf[...], pair, preferred_element_type=F32)
            r.ps_buf[z, :, q * W : (q + 2) * W] = part.astype(BF16)
        x_out(k).start()
        if k > 0:
            spread(k - 1)
        if k == 1:
            relay_diag(dn, HI - 1)
    spread(HI - 1)

    @pl.when(edge)
    def _():
        for k in range(HI):
            p_out(order(k), near).start()

    def drain():
        for z in range(1, HI):

            @pl.when(hi + z < HI)
            def _():
                sent(r.kv_buf.at[0], r.k_send.at[z])
                sent(r.bias_in.at[0], r.b_send.at[z])

        sent(r.kv_buf.at[0, pl.ds(0, (LO - 1) * T)], r.k_send.at[0])
        sent(r.bias_in.at[0, pl.ds(0, LO - 1)], r.b_send.at[0])
        sent(r.q_in.at[pl.ds(0, LO - 1)], r.q_send.at[0])
        sent(r.att_pl.at[pl.ds(0, (LO - 1) * T)], r.t_send.at[0])
        sent(up.blocks(HI - 1), r.wz_send.at[0])
        sent(dn.blocks(HI - 1), r.wz_send.at[1])
        up.wait_sent(HI)
        dn.wait_sent(HI)
        for z in range(HI):

            @pl.when((z <= hi) & (hi + 1 < HI))
            def _():
                sent(r.res_buf, r.nu_send.at[z])

            @pl.when((z >= hi) & (hi > 0))
            def _():
                sent(r.res_buf, r.nd_send.at[z])

        sent(r.n_buf.at[pl.ds(0, HI * H)], r.np_send.at[0])
        sent(r.x_in, r.x_send.at[0])

    scoped("drain", drain)
    for k in range(HI):
        z = order(k)
        cols = pl.ds(pl.multiple_of(z * CW, LANES), CW)
        update = r.xs_buf[z, pl.ds(hi * H, H), :].astype(F32)
        scoped(f"sum_wait{k}", arrived, r.pr_buf.at[z, pl.ds(0, HI - 1)], r.p_recv.at[z])
        for far in range(1, HI):
            update = update + r.pr_buf[z, (hi + far) % HI].astype(F32)
        r.out_ref[:, cols] = (r.res_buf[:, cols].astype(F32) + update).astype(BF16)
    sent(r.pr_buf.at[:, pl.ds(0, HI - 1)], r.p_send.at[0])


def fits(tokens, queries, key_values, stop_bias, up_proj, down_proj):
    sp = lax.axis_size("sp")
    rows, seqs, heads = stop_bias.shape
    hidden = up_proj.shape[1]
    return (
        lax.axis_size("tp") == 2
        and sp == LO * LO
        and seqs == 1
        and heads == 2 * LO
        and queries.shape[2] == heads * HEAD
        and key_values.shape[2] == heads * HEAD
        and 2 * HEAD == LANES
        and 2 * rows == LANES
        and hidden % (sp // LO * LANES) == 0
        and down_proj.shape[1] % LANES == 0
        and up_proj.shape[0] % 16 == 0
        and tokens.shape[2] % 512 == 0
    )


def body(tokens, queries, key_values, stop_bias, out_proj, norm_gain, up_proj, down_proj):
    if not fits(tokens, queries, key_values, stop_bias, up_proj, down_proj):
        return general_body(
            tokens, queries, key_values, stop_bias, out_proj, norm_gain, up_proj, down_proj
        )
    sp = lax.axis_size("sp")
    HI = sp // LO
    T, _, D = tokens.shape
    H = T // 2
    heads = stop_bias.shape[2]
    G = heads // 2
    R, hidden = up_proj.shape
    CH = hidden // HI
    W = down_proj.shape[1]
    PL = LO * T
    NC = 4
    vmem = pl.BlockSpec(memory_space=pltpu.VMEM)
    hbm = pl.BlockSpec(memory_space=pl.ANY)

    def sem(*shape):
        return pltpu.SemaphoreType.DMA(shape)

    operands = dict(
        tok_hbm=(tokens.reshape(T, D), hbm),
        q_hbm=(queries.reshape(T, queries.shape[2]), hbm),
        kv_hbm=(key_values.reshape(T, key_values.shape[2]), hbm),
        bias_hbm=(stop_bias.reshape(T, heads).T, hbm),
        wo_hbm=(out_proj, hbm),
        gain_hbm=(norm_gain.reshape(1, D), hbm),
        up_hbm=(up_proj, hbm),
        dn_hbm=(down_proj, hbm),
    )
    scratch = dict(
        tok_v=pltpu.VMEM((T, D), BF16),
        bias_v=pltpu.VMEM((heads, T), BF16),
        q_v=pltpu.VMEM((T, G * LANES), BF16),
        kv_v=pltpu.VMEM((T, G * LANES), BF16),
        wo_v=pltpu.VMEM(out_proj.shape, BF16),
        gain_v=pltpu.VMEM((1, D), F32),
        up_v=pltpu.VMEM((R, hidden), BF16),
        dn_v=pltpu.VMEM((hidden, W), BF16),
        up_buf=pltpu.VMEM((sp * R, CH), BF16),
        dn_buf=pltpu.VMEM((sp, CH, W), BF16),
        bias_out=pltpu.VMEM((G, 2, LANES), F32),
        bias_in=pltpu.VMEM((HI, LO, 2, LANES), F32),
        bias_pl=pltpu.VMEM((HI, 2, PL), F32),
        q_in=pltpu.VMEM((LO, T, LANES), BF16),
        q_all=pltpu.VMEM((2 * PL, LANES), BF16),
        kv_buf=pltpu.VMEM((HI, PL, LANES), BF16),
        tri_buf=pltpu.VMEM((PL, PL + LANES), BF16),
        carry=pltpu.VMEM((2 * PL, LANES), F32),
        acc=pltpu.VMEM((2 * PL, LANES), F32),
        att_pl=pltpu.VMEM((PL, LANES), BF16),
        att_buf=pltpu.VMEM((T, G * LANES), BF16),
        pj_buf=pltpu.VMEM((T, D), BF16),
        pj_in=pltpu.VMEM((H, D), BF16),
        res_buf=pltpu.VMEM((H, D), BF16),
        n_buf=pltpu.VMEM((HI * T, D), BF16),
        hid_buf=pltpu.VMEM((HI * T, CH), BF16),
        ps_buf=pltpu.VMEM((HI, HI * T, LO * W), BF16),
        x_in=pltpu.VMEM((HI, HI * H, LO * W), BF16),
        xs_buf=pltpu.VMEM((HI, HI * H, LO * W), BF16),
        pr_buf=pltpu.VMEM((HI, HI, H, LO * W), BF16),
        load_sem=sem(10),
        k_send=sem(HI),
        b_send=sem(HI),
        ready=pltpu.SemaphoreType.REGULAR,
        q_send=sem(1),
        k_recv=sem(HI),
        b_recv=sem(HI),
        q_recv=sem(1),
        wz_send=sem(2),
        up_sp=sem(1),
        up_own=sem(HI),
        up_near=sem(HI),
        up_diag=sem(HI),
        dn_sp=sem(1),
        dn_own=sem(HI),
        dn_near=sem(HI),
        dn_diag=sem(HI),
        t_send=sem(1),
        t_recv=sem(1),
        pj_send=pltpu.SemaphoreType.DMA,
        pj_recv=pltpu.SemaphoreType.DMA,
        nu_send=sem(HI),
        nd_send=sem(HI),
        np_send=sem(1),
        nz_recv=sem(HI * NC),
        nc_recv=sem(1),
        x_send=sem(1),
        x_recv=sem(HI),
        p_send=sem(1),
        p_recv=sem(HI),
    )
    names = [*operands, "out_ref", *scratch]
    out = pl.pallas_call(
        lambda *refs: layer_kernel(HI, G, NC, names, *refs),
        out_shape=pltpu.VMEM((H, D), BF16),
        in_specs=[spec for _, spec in operands.values()],
        out_specs=vmem,
        scratch_shapes=list(scratch.values()),
        compiler_params=pltpu.CompilerParams(
            collective_id=0, has_side_effects=True, vmem_limit_bytes=56 * 1024 * 1024
        ),
        name="layer",
    )(*[value for value, _ in operands.values()])
    return out.reshape(H, 1, D)


def solution(mesh):
    return jax.shard_map(
        body,
        mesh=mesh,
        in_specs=(
            P("sp", None, None),
            P("sp", None, "tp"),
            P("sp", None, "tp"),
            P("sp", None, "tp"),
            P("tp", None),
            P(),
            P("sp", "tp"),
            P("tp", "sp"),
        ),
        out_specs=P(("sp", "tp"), None, None),
        check_vma=False,
    )
```

```python
import math

import jax
import jax.numpy as jnp
from jax import lax
from jax.experimental import pallas as pl
from jax.experimental.pallas import tpu as pltpu
from jax.sharding import PartitionSpec as P

HEAD = 64


EPSILON = 1e-06


def rms_scale(residual, gain):
    values = residual.astype(jnp.float32)
    factor = lax.rsqrt(jnp.mean(values * values, axis=-1, keepdims=True) + EPSILON)
    return (values * factor * gain).astype(jnp.bfloat16)


def sweep_keys(totals, pieces, shard_rows, step_fn):
    kv_rows, bias_rows = pieces
    shards = kv_rows.shape[0] // shard_rows
    group_shards = math.gcd(shards, max(1, 1024 // shard_rows))
    span_rows = group_shards * shard_rows

    def advance(number, running):
        first_row = number * span_rows
        kv_block = lax.dynamic_slice_in_dim(kv_rows, first_row, span_rows, 0)
        bias_block = lax.dynamic_slice_in_dim(bias_rows, first_row, span_rows, 0)
        return step_fn(running, kv_block, bias_block, first_row, group_shards)

    return lax.fori_loop(0, shards // group_shards, advance, totals)


def general_body(tokens, queries, key_values, stop_bias, out_proj, norm_gain, up_proj, down_proj):
    row_count = tokens.shape[0]
    seq_count = tokens.shape[1]
    head_count = queries.shape[2] // HEAD
    kv_count = key_values.shape[2] // (2 * HEAD)
    group_size = head_count // kv_count
    n_shards = lax.axis_size("sp")
    query_start = lax.axis_index("sp") * row_count
    query_pos = query_start + lax.iota(jnp.int32, row_count)
    q_heads = queries.reshape(row_count, seq_count, kv_count, group_size, HEAD).transpose(
        1, 2, 3, 0, 4
    )
    q_heads = q_heads.reshape(seq_count, kv_count, group_size * row_count, HEAD)

    def stick_block(kv_block, bias_block, key_start):
        span_rows = kv_block.shape[0]
        key_pairs = kv_block.reshape(span_rows, seq_count, kv_count, 2 * HEAD)
        keys_part = key_pairs[..., :HEAD]
        values_part = key_pairs[..., HEAD:]
        scores = (
            jnp.einsum("bgmd,sbgd->bgms", q_heads, keys_part, preferred_element_type=jnp.float32)
            * 0.125
        )
        bias_float = jnp.transpose(bias_block, (1, 2, 0)).astype(jnp.float32)
        scores = (
            scores.reshape(seq_count, head_count, row_count, span_rows) + bias_float[:, :, None, :]
        )
        key_pos = key_start + lax.iota(jnp.int32, span_rows)
        strict = key_pos[None, :] < query_pos[:, None]
        log_pass = jnp.where(strict, jax.nn.log_sigmoid(-scores), 0.0)
        return (scores, strict, log_pass, values_part)

    def weigh(scores, strict, after_sum, values_part):
        span_rows = scores.shape[3]
        weights = jnp.where(strict, jnp.exp(jax.nn.log_sigmoid(scores) + after_sum), 0.0).astype(
            jnp.bfloat16
        )
        weights = weights.reshape(seq_count, kv_count, group_size * row_count, span_rows)
        return jnp.einsum(
            "bgms,sbgd->bgmd", weights, values_part, preferred_element_type=jnp.float32
        )

    empty_out = jnp.zeros((seq_count, kv_count, group_size * row_count, HEAD), jnp.float32)

    def sum_step(sums_table, kv_block, bias_block, key_start, shard_group):

        def sum_compute(table_in):
            scores, strict, log_pass, values_part = stick_block(kv_block, bias_block, key_start)
            block_sums = log_pass.reshape(
                seq_count, head_count, row_count, shard_group, row_count
            ).sum(axis=4)
            slot_index = key_start // row_count
            current = lax.dynamic_slice_in_dim(table_in, slot_index, shard_group, 0)
            return lax.dynamic_update_slice_in_dim(
                table_in, current + jnp.transpose(block_sums, (3, 0, 1, 2)), slot_index, 0
            )

        return lax.cond(
            key_start < query_start + row_count, sum_compute, lambda table_in: table_in, sums_table
        )

    empty_table = jnp.zeros((n_shards, seq_count, head_count, row_count), jnp.float32)
    sums_table = sweep_keys(
        empty_table,
        (
            lax.all_gather(key_values, "sp", axis=0, tiled=True),
            lax.all_gather(stop_bias, "sp", axis=0, tiled=True),
        ),
        row_count,
        sum_step,
    )
    offsets = lax.cumsum(sums_table, axis=0, reverse=True) - sums_table

    def out_step(outputs, kv_block, bias_block, key_start, shard_group):

        def out_compute(running):
            scores, strict, log_pass, values_part = stick_block(kv_block, bias_block, key_start)
            span_rows = kv_block.shape[0]
            split_pass = log_pass.reshape(seq_count, head_count, row_count, shard_group, row_count)
            within = lax.cumsum(split_pass, axis=4, reverse=True) - split_pass
            carried = lax.dynamic_slice_in_dim(offsets, key_start // row_count, shard_group, 0)
            carried = jnp.transpose(carried, (1, 2, 3, 0))[..., None]
            after_sum = (within + carried).reshape(seq_count, head_count, row_count, span_rows)
            return running + weigh(scores, strict, after_sum, values_part)

        return lax.cond(
            key_start < query_start + row_count, out_compute, lambda running: running, outputs
        )

    accum_out = sweep_keys(
        empty_out,
        (
            lax.all_gather(key_values, "sp", axis=0, tiled=True),
            lax.all_gather(stop_bias, "sp", axis=0, tiled=True),
        ),
        row_count,
        out_step,
    )
    attended = accum_out.reshape(seq_count, kv_count, group_size, row_count, HEAD).transpose(
        3, 0, 1, 2, 4
    )
    attended = attended.reshape(row_count * seq_count, head_count * HEAD).astype(jnp.bfloat16)
    share_tokens = row_count // lax.axis_size("tp")
    share_rows = share_tokens * seq_count
    tp_index = lax.axis_index("tp")
    projected = lax.psum(
        jnp.dot(attended, out_proj, preferred_element_type=jnp.float32).astype(jnp.bfloat16), "tp"
    ).astype(jnp.float32)
    flat_tokens = tokens.reshape(row_count * seq_count, tokens.shape[2])
    residual = (flat_tokens.astype(jnp.float32) + projected).astype(jnp.bfloat16)
    normed = rms_scale(residual, norm_gain)
    residual_share = lax.dynamic_slice_in_dim(residual, tp_index * share_rows, share_rows, 0)
    up_values = jnp.dot(
        normed,
        lax.all_gather(up_proj, "sp", axis=0, tiled=True),
        preferred_element_type=jnp.float32,
    )
    hidden = jnp.square(jax.nn.relu(up_values)).astype(jnp.bfloat16)
    partial_terms = jnp.dot(
        hidden,
        lax.all_gather(down_proj, "sp", axis=1, tiled=True),
        preferred_element_type=jnp.float32,
    )
    update = lax.psum_scatter(
        partial_terms.astype(jnp.bfloat16), "tp", scatter_dimension=0, tiled=True
    ).astype(jnp.float32)
    result = (residual_share.astype(jnp.float32) + update).astype(jnp.bfloat16)
    return result.reshape(share_tokens, seq_count, result.shape[1])


MESH = pl.DeviceIdType.MESH
LO = 4
LANES = 128
F32 = jnp.float32
BF16 = jnp.bfloat16


def remote(src, dst, send, recv, sp, tp):
    return pltpu.make_async_remote_copy(
        src_ref=src,
        dst_ref=dst,
        send_sem=send,
        recv_sem=recv,
        device_id={"sp": sp, "tp": tp},
        device_id_type=MESH,
    )


def dot_nt(a, b):
    return lax.dot_general(a, b, (((1,), (1,)), ((), ())), preferred_element_type=F32)


def dot_tn(a, b):
    return lax.dot_general(a, b, (((0,), (0,)), ((), ())), preferred_element_type=F32)


class Refs:
    def __init__(self, names, refs):
        for name, ref in zip(names, refs):
            setattr(self, name, ref)


class Piece:
    def __init__(self, place, view, blocks, rows, sem):
        self.view, self.blocks, self.rows = view, blocks, rows
        self.send, self.own, self.near, self.far = sem
        self.s, self.c, self.hi, self.lo, self.lo1, self.lo2, self.lo3 = place

    def full(self, j):
        return self.view(j, 0, self.rows)

    def part(self, j, h):
        return self.view(j, h * (self.rows // 2), self.rows // 2)

    def direct(self, z, src=None):
        j = z * LO + self.lo
        src = self.full(j) if src is None else src
        return [
            remote(src, self.full(j), self.send.at[0], self.near.at[z], self.hi * LO + p, self.c)
            for p in (self.lo1, self.lo2)
        ]

    def diag(self, z):
        first, last = self.part(z * LO + self.lo1, 0), self.part(z * LO + self.lo2, 1)
        return [
            remote(first, first, self.send.at[0], self.far.at[z], self.hi * LO + self.lo2, self.c),
            remote(last, last, self.send.at[0], self.far.at[z], self.hi * LO + self.lo1, self.c),
        ]

    def arrived(self, ref, sem):
        remote(ref, ref, self.send.at[0], sem, self.s, 1 - self.c).wait_recv()

    def wait_own(self, z):
        self.arrived(self.full(z * LO + self.lo), self.own.at[z])

    def wait_direct(self, z):
        self.arrived(self.blocks(2), self.near.at[z])

    def wait_diag(self, z):
        self.arrived(self.full(z * LO + self.lo3), self.far.at[z])

    def wait_sent(self, planes):
        ref = self.blocks(3 * planes)
        remote(ref, ref, self.send.at[0], self.far.at[0], self.s, 1 - self.c).wait_send()


def start(copies):
    for copy in copies:
        copy.start()


def scoped(name, fn, *args):
    with jax.named_scope(name):
        return fn(*args)


def layer_kernel(HI, G, NC, names, *refs):
    r = Refs(names, refs)
    s = lax.axis_index("sp")
    c = lax.axis_index("tp")
    hi = s // LO
    lo = s % LO
    lo1 = lo + 1 - 2 * (lo % 2)
    lo2 = (lo + 2) % LO
    lo3 = (lo1 + 2) % LO
    other = 1 - c
    peers = (lo1, lo2, lo3)
    T = r.q_v.shape[0]
    H = T // 2
    D = r.tok_v.shape[1]
    R = r.up_v.shape[0]
    CH = r.up_buf.shape[1]
    W = r.dn_v.shape[1]
    PL = LO * T
    QR = 2 * PL
    own_cols = pl.ds(pl.multiple_of(hi * CH, LANES), CH)
    own_lanes = pl.ds(pl.multiple_of(lo * LANES, LANES), LANES)

    barrier = pltpu.get_barrier_semaphore()
    for p in peers:
        pl.semaphore_signal(barrier, inc=1, device_id={"sp": hi * LO + p, "tp": c}, device_id_type=MESH)
    pl.semaphore_signal(barrier, inc=1, device_id={"sp": s, "tp": other}, device_id_type=MESH)
    for dz in range(1, HI):
        far = ((hi + dz) % HI) * LO + lo
        pl.semaphore_signal(barrier, inc=1, device_id={"sp": far, "tp": c}, device_id_type=MESH)
    local = [
        (r.bias_hbm, r.bias_v),
        (r.kv_hbm, r.kv_v),
        (r.q_hbm, r.q_v),
        (r.up_hbm, r.up_v),
        (r.dn_hbm, r.dn_v),
        (r.up_hbm.at[:, own_cols], r.up_buf.at[pl.ds(s * R, R)]),
        (r.dn_hbm.at[pl.ds(hi * CH, CH)], r.dn_buf.at[s]),
        (r.tok_hbm, r.tok_v),
        (r.wo_hbm, r.wo_v),
        (r.gain_hbm, r.gain_v),
    ]
    loads = [pltpu.make_async_copy(a, b, r.load_sem.at[i]) for i, (a, b) in enumerate(local)]
    start(loads[:5])
    loads[0].wait()

    half_lane = lax.broadcasted_iota(jnp.int32, (2 * G, LANES), 1) // HEAD
    bias = r.bias_v[...].astype(F32)
    bias = jnp.where(half_lane == lo % 2, jnp.concatenate([bias, bias], axis=1), 0.0)
    for g in range(G):
        r.bias_out[g] = bias[2 * g : 2 * g + 2]
    with jax.named_scope("barrier"):
        for load in loads[1:3]:
            load.wait()
        pl.semaphore_wait(barrier, 4 + (HI - 1))

    place = (s, c, hi, lo, lo1, lo2, lo3)
    up = Piece(
        place,
        lambda j, a, n: r.up_buf.at[pl.ds(j * R + a, n)],
        lambda n: r.up_buf.at[pl.ds(0, n * R)],
        R,
        (r.up_sp, r.up_own, r.up_near, r.up_diag),
    )
    dn = Piece(
        place,
        lambda j, a, n: r.dn_buf.at[j, pl.ds(a, n)],
        lambda n: r.dn_buf.at[pl.ds(0, n)],
        CH,
        (r.dn_sp, r.dn_own, r.dn_near, r.dn_diag),
    )

    def arrived(ref, sem):
        remote(ref, ref, r.pj_send, sem, s, other).wait_recv()

    def sent(ref, sem):
        remote(ref, ref, sem, r.pj_recv, s, other).wait_send()

    def send_keys(d, p):
        lanes = pl.ds(pl.multiple_of(p * LANES, LANES), LANES)
        dev = (hi + d) * LO + p
        return [
            remote(r.kv_v.at[:, lanes], r.kv_buf.at[hi, pl.ds(lo * T, T)], r.k_send.at[d], r.k_recv.at[hi], dev, c),
            remote(r.bias_out.at[p], r.bias_in.at[hi, lo], r.b_send.at[d], r.b_recv.at[hi], dev, c),
        ]

    def send_queries(p):
        lanes = pl.ds(pl.multiple_of(p * LANES, LANES), LANES)
        return remote(r.q_v.at[:, lanes], r.q_in.at[lo], r.q_send.at[0], r.q_recv.at[0], hi * LO + p, c)

    def keys_of(z, shards):
        arrived(r.kv_buf.at[z, pl.ds(0, shards * T)], r.k_recv.at[z])
        arrived(r.bias_in.at[z, pl.ds(0, shards)], r.b_recv.at[z])

    def join_bias(z):
        for i in range(LO // 2):
            r.bias_pl[z, :, i * LANES : (i + 1) * LANES] = r.bias_in[z, 2 * i] + r.bias_in[z, 2 * i + 1]

    def up_far(hp):
        cols = pl.ds(pl.multiple_of(hp * CH, LANES), CH)
        return remote(r.up_v.at[:, cols], up.full(s), r.wz_send.at[0], r.up_own.at[hi], hp * LO + lo, c)

    def dn_far(hp):
        rows = pl.ds(hp * CH, CH)
        return remote(r.dn_v.at[rows], dn.full(s), r.wz_send.at[1], r.dn_own.at[hi], hp * LO + lo, c)

    small = jnp.minimum(hi, HI - 1 - hi)
    tilt = jnp.where(hi <= HI - 1 - hi, 1, -1)

    def nth(k):
        if k == 0:
            return hi
        near = hi + (k + 1) // 2 if k % 2 else hi - k // 2
        return jnp.where(k <= 2 * small, near, hi + tilt * (k - small))

    upper = hi // (HI // 2)
    rank = hi + upper * (HI - 1 - 2 * hi)

    def order(k):
        if k == 0:
            return hi
        z = k - 1 + (rank < k).astype(jnp.int32)
        return z + upper * (HI - 1 - 2 * z)

    def below(far, d):
        @pl.when(hi >= d)
        def _():
            far(hi - d).start()

    def above(far, d):
        @pl.when(hi + d < HI)
        def _():
            far(hi + d).start()

    for p in peers:
        pl.semaphore_signal(r.ready, inc=1, device_id={"sp": hi * LO + p, "tp": c}, device_id_type=MESH)
    for p in peers:
        start(send_keys(0, p))
        send_queries(p).start()

    def raise_keys(shards):
        for d in range(HI - 1, 0, -1):

            @pl.when(hi + d < HI)
            def _():
                for p in shards:
                    start(send_keys(d, p))

    raise_keys((lo,))
    start(loads[5:])
    for load in loads[3:5]:
        load.wait()
    pair = hi + 1 - 2 * (hi % 2)
    for d in range(1, HI):
        below(up_far, d)
        if d == 1:
            pl.when(hi % 2 == 1)(lambda: dn_far(pair).start())
    scoped("ready", pl.semaphore_wait, r.ready, LO - 1)
    raise_keys(peers)
    start(up.direct(hi, r.up_v.at[:, own_cols]))
    for d in range(1, HI):
        above(up_far, d)
        if d == 1:
            pl.when(hi % 2 == 0)(lambda: dn_far(pair).start())
    start(dn.direct(hi, r.dn_v.at[pl.ds(hi * CH, CH)]))

    r.q_in[lo] = r.q_v[:, own_lanes]
    r.kv_buf[hi, pl.ds(lo * T, T), :] = r.kv_v[:, own_lanes]
    r.bias_in[hi, lo] = r.bias_out[lo]
    row_id = lax.broadcasted_iota(jnp.int32, (PL, PL + LANES), 0)
    col_id = lax.broadcasted_iota(jnp.int32, (PL, PL + LANES), 1)
    after_key = (row_id > col_id) | (col_id >= PL)
    r.tri_buf[...] = jnp.where(after_key, 1.0, 0.0).astype(BF16)
    low = lax.broadcasted_iota(jnp.int32, (T, LANES), 1) < HEAD

    with jax.named_scope("heads_wait"):
        keys_of(hi, LO - 1)
        arrived(r.q_in.at[pl.ds(0, LO - 1)], r.q_recv.at[0])
    join_bias(hi)
    for j in range(LO):
        qg = r.q_in[j].astype(F32) * 0.125
        r.q_all[j * T : (j + 1) * T] = jnp.where(low, qg, 0.0).astype(BF16)
        r.q_all[PL + j * T : PL + (j + 1) * T] = jnp.where(low, pltpu.roll(qg, HEAD, 1), 0.0).astype(BF16)

    step = 128

    def attend(z, own):
        keys = r.kv_buf[z]
        for i in range(QR // step):
            rows = slice(i * step, (i + 1) * step)
            head = i * step // PL
            scores = dot_nt(r.q_all[rows], keys) + r.bias_pl[z, head : head + 1, :]
            soft = jnp.maximum(scores, 0.0) + jnp.log(1.0 + jnp.exp(-jnp.abs(scores)))
            log_pass = -soft
            if own:
                query = i * step % PL + lax.broadcasted_iota(jnp.int32, (step, PL), 0)
                strict = lax.broadcasted_iota(jnp.int32, (step, PL), 1) < query
                log_pass = jnp.where(strict, log_pass, 0.0)
            top = log_pass.astype(BF16)
            rest = (log_pass - top.astype(F32)).astype(BF16)
            sums = jnp.dot(top, r.tri_buf[...], preferred_element_type=F32) + jnp.dot(
                rest, r.tri_buf[...], preferred_element_type=F32
            )
            power = scores - soft + sums[:, :PL]
            if not own:
                held = r.carry[rows]
                power = power + jnp.concatenate([held] * (PL // LANES), axis=1)
            weights = jnp.exp(power)
            if own:
                weights = jnp.where(strict, weights, 0.0)
            part = jnp.dot(weights.astype(BF16), keys, preferred_element_type=F32)
            if own:
                r.acc[rows] = part
                r.carry[rows] = sums[:, PL:]
            else:
                r.acc[rows] += part
                r.carry[rows] = held + sums[:, PL:]

    def look(d):
        @pl.when(hi >= d)
        def _():
            z = hi - d
            scoped(f"keys_wait{d}", keys_of, z, LO)
            join_bias(z)
            scoped(f"attend{d}", attend, z, False)

    def relay_direct(piece, k):
        z = nth(k) if piece is up else order(k)
        scoped(f"{'UD'[piece is dn]}own_wait{k}", piece.wait_own, z)
        start(piece.direct(z))

    def relay_diag(piece, k):
        z = nth(k) if piece is up else order(k)
        scoped(f"{'UD'[piece is dn]}direct_wait{k}", piece.wait_direct, z)
        start(piece.diag(z))

    scoped("attend0", attend, hi, True)
    relay_diag(up, 0)
    for d in range(1, HI):
        look(d)
        if d == 1:
            relay_direct(up, 1)

    heads = [r.acc[h * PL : (h + 1) * PL] for h in range(2)]
    low_pl = lax.broadcasted_iota(jnp.int32, (PL, LANES), 1) < HEAD
    r.att_pl[...] = jnp.where(low_pl, pltpu.roll(heads[0], HEAD, 1), heads[1]).astype(BF16)

    def att_back(p):
        src = r.att_pl.at[pl.ds(p * T, T)]
        return remote(src, r.att_buf.at[:, own_lanes], r.t_send.at[0], r.t_recv.at[0], hi * LO + p, c)

    for p in peers:
        att_back(p).start()

    def dn_below():
        for d in range(1, HI):

            @pl.when((hi >= d) & (hi - d != pair))
            def _():
                dn_far(hi - d).start()

    def dn_above():
        for d in range(1, HI):

            @pl.when((hi + d < HI) & (hi + d != pair))
            def _():
                dn_far(hi + d).start()

    dn_below()
    pl.when(hi == 0)(dn_above)
    r.att_buf[:, own_lanes] = r.att_pl[pl.ds(lo * T, T), :]
    relay_diag(dn, 0)
    pl.when(upper == 0)(lambda: relay_direct(up, 2))
    with jax.named_scope("att_wait"):
        for load in loads[5:]:
            load.wait()
        arrived(r.att_pl.at[pl.ds(0, (LO - 1) * T)], r.t_recv.at[0])

    att = r.att_buf[...]
    wide = 512 if D % 512 == 0 else LANES
    for i in range(D // wide):
        cols = slice(i * wide, (i + 1) * wide)
        r.pj_buf[:, cols] = jnp.dot(att, r.wo_v[:, cols], preferred_element_type=F32).astype(BF16)
    pj_copy = remote(r.pj_buf.at[pl.ds(other * H, H)], r.pj_in, r.pj_send, r.pj_recv, s, other)
    pj_copy.start()
    pl.when(hi > 0)(dn_above)
    relay_diag(up, 1)
    relay_direct(dn, 1)
    pl.when(upper == 1)(lambda: relay_direct(up, 2))
    scoped("pj_wait", pj_copy.wait)
    mine = pl.ds(c * H, H)
    total = r.pj_buf[mine, :].astype(F32) + r.pj_in[...].astype(F32)
    residual = (r.tok_v[mine, :].astype(F32) + total).astype(BF16)
    r.res_buf[...] = residual
    values = residual.astype(F32)
    factor = lax.rsqrt(jnp.mean(values * values, axis=-1, keepdims=True) + EPSILON)
    r.n_buf[pl.ds((c * HI + hi) * H, H), :] = (values * factor * r.gain_v[...]).astype(BF16)

    NW = D // NC

    def n_at(z, core, q):
        return r.n_buf.at[pl.ds((core * HI + z) * H, H), q * NW : (q + 1) * NW]

    def n_up(z, q):
        return remote(n_at(z, c, q), n_at(z, c, q), r.nu_send.at[z], r.nz_recv.at[z * NC + q], s + LO, c)

    def n_down(z, q):
        return remote(n_at(z, c, q), n_at(z, c, q), r.nd_send.at[z], r.nz_recv.at[z * NC + q], s - LO, c)

    def n_pass(z, q):
        return remote(n_at(z, c, q), n_at(z, c, q), r.np_send.at[0], r.nc_recv.at[0], s, other)

    for q in range(NC):

        @pl.when(hi + 1 < HI)
        def _():
            n_up(hi, q).start()

        @pl.when(hi > 0)
        def _():
            n_down(hi, q).start()

    for q in range(NC):
        n_pass(hi, q).start()

    def norm_take(k):
        z = order(k)
        for q in range(NC):
            scoped(f"norm_wait{k}", arrived, n_at(z, c, q), r.nz_recv.at[z * NC + q])

            @pl.when((z < hi) & (hi + 1 < HI))
            def _():
                n_up(z, q).start()

            @pl.when((z > hi) & (hi > 0))
            def _():
                n_down(z, q).start()

            n_pass(z, q).start()

    relay_direct(up, 3)
    relay_diag(up, 2)
    relay_diag(dn, 1)
    norm_take(1)
    relay_diag(up, 3)
    relay_direct(dn, 2)
    norm_take(2)
    relay_direct(dn, 3)
    norm_take(3)
    relay_diag(dn, 2)
    with jax.named_scope("norm_other_wait"):
        arrived(r.n_buf.at[pl.ds(0, HI * H)], r.nc_recv.at[0])
    with jax.named_scope("up_wait"):
        for k in range(HI):
            up.wait_diag(nth(k))

    wide = 256 if CH % 256 == 0 else LANES
    for i in range(CH // wide):
        cols = slice(i * wide, (i + 1) * wide)
        raw = jnp.maximum(jnp.dot(r.n_buf[...], r.up_buf[:, cols], preferred_element_type=F32), 0.0)
        r.hid_buf[:, cols] = (raw * raw).astype(BF16)
    half = HI * H
    CW = LO * W
    mine_rows = pl.ds(c * half, half)

    def x_out(k):
        z = order(k)
        rows = pl.ds(other * half, half)
        return remote(r.ps_buf.at[z, rows], r.x_in.at[z], r.x_send.at[0], r.x_recv.at[z], s, other)

    edge = (hi == 0) | (hi == HI - 1)
    near = hi + 1 - 2 * (hi % 2)
    away = (1 - upper) * (HI - 1)
    middle = away + 2 * upper - 1

    def p_out(z, hp):
        return remote(r.xs_buf.at[z, pl.ds(hp * H, H)], r.pr_buf.at[z, hi], r.p_send.at[0], r.p_recv.at[z], hp * LO + lo, c)

    def spread(k):
        z = order(k)
        scoped(f"x_wait{k}", arrived, r.x_in.at[z], r.x_recv.at[z])
        mixed = r.ps_buf[z, mine_rows, :].astype(F32) + r.x_in[z].astype(F32)
        r.xs_buf[z] = mixed.astype(BF16)

        p_out(z, away).start()
        p_out(z, middle).start()
        pl.when(jnp.logical_not(edge))(lambda: p_out(z, near).start())

    for k in range(HI):
        z = order(k)
        scoped(f"dn_wait{k}", dn.wait_diag, z)
        for q in range(0, LO, 2):
            pair = jnp.concatenate([r.dn_buf[z * LO + q], r.dn_buf[z * LO + q + 1]], axis=1)
            part = jnp.dot(r.hid_buf[...], pair, preferred_element_type=F32)
            r.ps_buf[z, :, q * W : (q + 2) * W] = part.astype(BF16)
        x_out(k).start()
        if k > 0:
            spread(k - 1)
        if k == 1:
            relay_diag(dn, HI - 1)
    spread(HI - 1)

    @pl.when(edge)
    def _():
        for k in range(HI):
            p_out(order(k), near).start()

    def drain():
        for z in range(1, HI):

            @pl.when(hi + z < HI)
            def _():
                sent(r.kv_buf.at[0], r.k_send.at[z])
                sent(r.bias_in.at[0], r.b_send.at[z])

        sent(r.kv_buf.at[0, pl.ds(0, (LO - 1) * T)], r.k_send.at[0])
        sent(r.bias_in.at[0, pl.ds(0, LO - 1)], r.b_send.at[0])
        sent(r.q_in.at[pl.ds(0, LO - 1)], r.q_send.at[0])
        sent(r.att_pl.at[pl.ds(0, (LO - 1) * T)], r.t_send.at[0])
        sent(up.blocks(HI - 1), r.wz_send.at[0])
        sent(dn.blocks(HI - 1), r.wz_send.at[1])
        up.wait_sent(HI)
        dn.wait_sent(HI)
        for z in range(HI):

            @pl.when((z <= hi) & (hi + 1 < HI))
            def _():
                sent(r.res_buf, r.nu_send.at[z])

            @pl.when((z >= hi) & (hi > 0))
            def _():
                sent(r.res_buf, r.nd_send.at[z])

        sent(r.n_buf.at[pl.ds(0, HI * H)], r.np_send.at[0])
        sent(r.x_in, r.x_send.at[0])

    scoped("drain", drain)
    for k in range(HI):
        z = order(k)
        cols = pl.ds(pl.multiple_of(z * CW, LANES), CW)
        update = r.xs_buf[z, pl.ds(hi * H, H), :].astype(F32)
        scoped(f"sum_wait{k}", arrived, r.pr_buf.at[z, pl.ds(0, HI - 1)], r.p_recv.at[z])
        for far in range(1, HI):
            update = update + r.pr_buf[z, (hi + far) % HI].astype(F32)
        r.out_ref[:, cols] = (r.res_buf[:, cols].astype(F32) + update).astype(BF16)
    sent(r.pr_buf.at[:, pl.ds(0, HI - 1)], r.p_send.at[0])


def fits(tokens, queries, key_values, stop_bias, up_proj, down_proj):
    sp = lax.axis_size("sp")
    rows, seqs, heads = stop_bias.shape
    hidden = up_proj.shape[1]
    return (
        lax.axis_size("tp") == 2
        and sp == LO * LO
        and seqs == 1
        and heads == 2 * LO
        and queries.shape[2] == heads * HEAD
        and key_values.shape[2] == heads * HEAD
        and 2 * HEAD == LANES
        and 2 * rows == LANES
        and hidden % (sp // LO * LANES) == 0
        and down_proj.shape[1] % LANES == 0
        and up_proj.shape[0] % 16 == 0
        and tokens.shape[2] % 512 == 0
    )


def body(tokens, queries, key_values, stop_bias, out_proj, norm_gain, up_proj, down_proj):
    if not fits(tokens, queries, key_values, stop_bias, up_proj, down_proj):
        return general_body(
            tokens, queries, key_values, stop_bias, out_proj, norm_gain, up_proj, down_proj
        )
    sp = lax.axis_size("sp")
    HI = sp // LO
    T, _, D = tokens.shape
    H = T // 2
    heads = stop_bias.shape[2]
    G = heads // 2
    R, hidden = up_proj.shape
    CH = hidden // HI
    W = down_proj.shape[1]
    PL = LO * T
    NC = 4
    vmem = pl.BlockSpec(memory_space=pltpu.VMEM)
    hbm = pl.BlockSpec(memory_space=pl.ANY)

    def sem(*shape):
        return pltpu.SemaphoreType.DMA(shape)

    operands = dict(
        tok_hbm=(tokens.reshape(T, D), hbm),
        q_hbm=(queries.reshape(T, queries.shape[2]), hbm),
        kv_hbm=(key_values.reshape(T, key_values.shape[2]), hbm),
        bias_hbm=(stop_bias.reshape(T, heads).T, hbm),
        wo_hbm=(out_proj, hbm),
        gain_hbm=(norm_gain.reshape(1, D), hbm),
        up_hbm=(up_proj, hbm),
        dn_hbm=(down_proj, hbm),
    )
    scratch = dict(
        tok_v=pltpu.VMEM((T, D), BF16),
        bias_v=pltpu.VMEM((heads, T), BF16),
        q_v=pltpu.VMEM((T, G * LANES), BF16),
        kv_v=pltpu.VMEM((T, G * LANES), BF16),
        wo_v=pltpu.VMEM(out_proj.shape, BF16),
        gain_v=pltpu.VMEM((1, D), F32),
        up_v=pltpu.VMEM((R, hidden), BF16),
        dn_v=pltpu.VMEM((hidden, W), BF16),
        up_buf=pltpu.VMEM((sp * R, CH), BF16),
        dn_buf=pltpu.VMEM((sp, CH, W), BF16),
        bias_out=pltpu.VMEM((G, 2, LANES), F32),
        bias_in=pltpu.VMEM((HI, LO, 2, LANES), F32),
        bias_pl=pltpu.VMEM((HI, 2, PL), F32),
        q_in=pltpu.VMEM((LO, T, LANES), BF16),
        q_all=pltpu.VMEM((2 * PL, LANES), BF16),
        kv_buf=pltpu.VMEM((HI, PL, LANES), BF16),
        tri_buf=pltpu.VMEM((PL, PL + LANES), BF16),
        carry=pltpu.VMEM((2 * PL, LANES), F32),
        acc=pltpu.VMEM((2 * PL, LANES), F32),
        att_pl=pltpu.VMEM((PL, LANES), BF16),
        att_buf=pltpu.VMEM((T, G * LANES), BF16),
        pj_buf=pltpu.VMEM((T, D), BF16),
        pj_in=pltpu.VMEM((H, D), BF16),
        res_buf=pltpu.VMEM((H, D), BF16),
        n_buf=pltpu.VMEM((HI * T, D), BF16),
        hid_buf=pltpu.VMEM((HI * T, CH), BF16),
        ps_buf=pltpu.VMEM((HI, HI * T, LO * W), BF16),
        x_in=pltpu.VMEM((HI, HI * H, LO * W), BF16),
        xs_buf=pltpu.VMEM((HI, HI * H, LO * W), BF16),
        pr_buf=pltpu.VMEM((HI, HI, H, LO * W), BF16),
        load_sem=sem(10),
        k_send=sem(HI),
        b_send=sem(HI),
        ready=pltpu.SemaphoreType.REGULAR,
        q_send=sem(1),
        k_recv=sem(HI),
        b_recv=sem(HI),
        q_recv=sem(1),
        wz_send=sem(2),
        up_sp=sem(1),
        up_own=sem(HI),
        up_near=sem(HI),
        up_diag=sem(HI),
        dn_sp=sem(1),
        dn_own=sem(HI),
        dn_near=sem(HI),
        dn_diag=sem(HI),
        t_send=sem(1),
        t_recv=sem(1),
        pj_send=pltpu.SemaphoreType.DMA,
        pj_recv=pltpu.SemaphoreType.DMA,
        nu_send=sem(HI),
        nd_send=sem(HI),
        np_send=sem(1),
        nz_recv=sem(HI * NC),
        nc_recv=sem(1),
        x_send=sem(1),
        x_recv=sem(HI),
        p_send=sem(1),
        p_recv=sem(HI),
    )
    names = [*operands, "out_ref", *scratch]
    out = pl.pallas_call(
        lambda *refs: layer_kernel(HI, G, NC, names, *refs),
        out_shape=pltpu.VMEM((H, D), BF16),
        in_specs=[spec for _, spec in operands.values()],
        out_specs=vmem,
        scratch_shapes=list(scratch.values()),
        compiler_params=pltpu.CompilerParams(
            collective_id=0, has_side_effects=True, vmem_limit_bytes=56 * 1024 * 1024
        ),
        name="layer",
    )(*[value for value, _ in operands.values()])
    return out.reshape(H, 1, D)


def solution(mesh):
    return jax.shard_map(
        body,
        mesh=mesh,
        in_specs=(
            P("sp", None, None),
            P("sp", None, "tp"),
            P("sp", None, "tp"),
            P("sp", None, "tp"),
            P("tp", None),
            P(),
            P("sp", "tp"),
            P("tp", "sp"),
        ),
        out_specs=P(("sp", "tp"), None, None),
        check_vma=False,
    )
```

```python
import math

import jax
import jax.numpy as jnp
from jax import lax
from jax.experimental import pallas as pl
from jax.experimental.pallas import tpu as pltpu
from jax.sharding import PartitionSpec as P

HEAD = 64


EPSILON = 1e-06


def rms_scale(residual, gain):
    values = residual.astype(jnp.float32)
    factor = lax.rsqrt(jnp.mean(values * values, axis=-1, keepdims=True) + EPSILON)
    return (values * factor * gain).astype(jnp.bfloat16)


def sweep_keys(totals, pieces, shard_rows, step_fn):
    kv_rows, bias_rows = pieces
    shards = kv_rows.shape[0] // shard_rows
    group_shards = math.gcd(shards, max(1, 1024 // shard_rows))
    span_rows = group_shards * shard_rows

    def advance(number, running):
        first_row = number * span_rows
        kv_block = lax.dynamic_slice_in_dim(kv_rows, first_row, span_rows, 0)
        bias_block = lax.dynamic_slice_in_dim(bias_rows, first_row, span_rows, 0)
        return step_fn(running, kv_block, bias_block, first_row, group_shards)

    return lax.fori_loop(0, shards // group_shards, advance, totals)


def general_body(tokens, queries, key_values, stop_bias, out_proj, norm_gain, up_proj, down_proj):
    row_count = tokens.shape[0]
    seq_count = tokens.shape[1]
    head_count = queries.shape[2] // HEAD
    kv_count = key_values.shape[2] // (2 * HEAD)
    group_size = head_count // kv_count
    n_shards = lax.axis_size("sp")
    query_start = lax.axis_index("sp") * row_count
    query_pos = query_start + lax.iota(jnp.int32, row_count)
    q_heads = queries.reshape(row_count, seq_count, kv_count, group_size, HEAD).transpose(
        1, 2, 3, 0, 4
    )
    q_heads = q_heads.reshape(seq_count, kv_count, group_size * row_count, HEAD)

    def stick_block(kv_block, bias_block, key_start):
        span_rows = kv_block.shape[0]
        key_pairs = kv_block.reshape(span_rows, seq_count, kv_count, 2 * HEAD)
        keys_part = key_pairs[..., :HEAD]
        values_part = key_pairs[..., HEAD:]
        scores = (
            jnp.einsum("bgmd,sbgd->bgms", q_heads, keys_part, preferred_element_type=jnp.float32)
            * 0.125
        )
        bias_float = jnp.transpose(bias_block, (1, 2, 0)).astype(jnp.float32)
        scores = (
            scores.reshape(seq_count, head_count, row_count, span_rows) + bias_float[:, :, None, :]
        )
        key_pos = key_start + lax.iota(jnp.int32, span_rows)
        strict = key_pos[None, :] < query_pos[:, None]
        log_pass = jnp.where(strict, jax.nn.log_sigmoid(-scores), 0.0)
        return (scores, strict, log_pass, values_part)

    def weigh(scores, strict, after_sum, values_part):
        span_rows = scores.shape[3]
        weights = jnp.where(strict, jnp.exp(jax.nn.log_sigmoid(scores) + after_sum), 0.0).astype(
            jnp.bfloat16
        )
        weights = weights.reshape(seq_count, kv_count, group_size * row_count, span_rows)
        return jnp.einsum(
            "bgms,sbgd->bgmd", weights, values_part, preferred_element_type=jnp.float32
        )

    empty_out = jnp.zeros((seq_count, kv_count, group_size * row_count, HEAD), jnp.float32)

    def sum_step(sums_table, kv_block, bias_block, key_start, shard_group):

        def sum_compute(table_in):
            scores, strict, log_pass, values_part = stick_block(kv_block, bias_block, key_start)
            block_sums = log_pass.reshape(
                seq_count, head_count, row_count, shard_group, row_count
            ).sum(axis=4)
            slot_index = key_start // row_count
            current = lax.dynamic_slice_in_dim(table_in, slot_index, shard_group, 0)
            return lax.dynamic_update_slice_in_dim(
                table_in, current + jnp.transpose(block_sums, (3, 0, 1, 2)), slot_index, 0
            )

        return lax.cond(
            key_start < query_start + row_count, sum_compute, lambda table_in: table_in, sums_table
        )

    empty_table = jnp.zeros((n_shards, seq_count, head_count, row_count), jnp.float32)
    sums_table = sweep_keys(
        empty_table,
        (
            lax.all_gather(key_values, "sp", axis=0, tiled=True),
            lax.all_gather(stop_bias, "sp", axis=0, tiled=True),
        ),
        row_count,
        sum_step,
    )
    offsets = lax.cumsum(sums_table, axis=0, reverse=True) - sums_table

    def out_step(outputs, kv_block, bias_block, key_start, shard_group):

        def out_compute(running):
            scores, strict, log_pass, values_part = stick_block(kv_block, bias_block, key_start)
            span_rows = kv_block.shape[0]
            split_pass = log_pass.reshape(seq_count, head_count, row_count, shard_group, row_count)
            within = lax.cumsum(split_pass, axis=4, reverse=True) - split_pass
            carried = lax.dynamic_slice_in_dim(offsets, key_start // row_count, shard_group, 0)
            carried = jnp.transpose(carried, (1, 2, 3, 0))[..., None]
            after_sum = (within + carried).reshape(seq_count, head_count, row_count, span_rows)
            return running + weigh(scores, strict, after_sum, values_part)

        return lax.cond(
            key_start < query_start + row_count, out_compute, lambda running: running, outputs
        )

    accum_out = sweep_keys(
        empty_out,
        (
            lax.all_gather(key_values, "sp", axis=0, tiled=True),
            lax.all_gather(stop_bias, "sp", axis=0, tiled=True),
        ),
        row_count,
        out_step,
    )
    attended = accum_out.reshape(seq_count, kv_count, group_size, row_count, HEAD).transpose(
        3, 0, 1, 2, 4
    )
    attended = attended.reshape(row_count * seq_count, head_count * HEAD).astype(jnp.bfloat16)
    share_tokens = row_count // lax.axis_size("tp")
    share_rows = share_tokens * seq_count
    tp_index = lax.axis_index("tp")
    projected = lax.psum(
        jnp.dot(attended, out_proj, preferred_element_type=jnp.float32).astype(jnp.bfloat16), "tp"
    ).astype(jnp.float32)
    flat_tokens = tokens.reshape(row_count * seq_count, tokens.shape[2])
    residual = (flat_tokens.astype(jnp.float32) + projected).astype(jnp.bfloat16)
    normed = rms_scale(residual, norm_gain)
    residual_share = lax.dynamic_slice_in_dim(residual, tp_index * share_rows, share_rows, 0)
    up_values = jnp.dot(
        normed,
        lax.all_gather(up_proj, "sp", axis=0, tiled=True),
        preferred_element_type=jnp.float32,
    )
    hidden = jnp.square(jax.nn.relu(up_values)).astype(jnp.bfloat16)
    partial_terms = jnp.dot(
        hidden,
        lax.all_gather(down_proj, "sp", axis=1, tiled=True),
        preferred_element_type=jnp.float32,
    )
    update = lax.psum_scatter(
        partial_terms.astype(jnp.bfloat16), "tp", scatter_dimension=0, tiled=True
    ).astype(jnp.float32)
    result = (residual_share.astype(jnp.float32) + update).astype(jnp.bfloat16)
    return result.reshape(share_tokens, seq_count, result.shape[1])


MESH = pl.DeviceIdType.MESH
LO = 4
LANES = 128
F32 = jnp.float32
BF16 = jnp.bfloat16


def remote(src, dst, send, recv, sp, tp):
    return pltpu.make_async_remote_copy(
        src_ref=src,
        dst_ref=dst,
        send_sem=send,
        recv_sem=recv,
        device_id={"sp": sp, "tp": tp},
        device_id_type=MESH,
    )


def dot_nt(a, b):
    return lax.dot_general(a, b, (((1,), (1,)), ((), ())), preferred_element_type=F32)


def dot_tn(a, b):
    return lax.dot_general(a, b, (((0,), (0,)), ((), ())), preferred_element_type=F32)


class Refs:
    def __init__(self, names, refs):
        for name, ref in zip(names, refs):
            setattr(self, name, ref)


class Piece:
    def __init__(self, place, view, blocks, rows, sem):
        self.view, self.blocks, self.rows = view, blocks, rows
        self.send, self.own, self.near, self.far = sem
        self.s, self.c, self.hi, self.lo, self.lo1, self.lo2, self.lo3 = place

    def full(self, j):
        return self.view(j, 0, self.rows)

    def part(self, j, h):
        return self.view(j, h * (self.rows // 2), self.rows // 2)

    def direct(self, z, src=None):
        j = z * LO + self.lo
        src = self.full(j) if src is None else src
        return [
            remote(src, self.full(j), self.send.at[0], self.near.at[z], self.hi * LO + p, self.c)
            for p in (self.lo1, self.lo2)
        ]

    def diag(self, z):
        first, last = self.part(z * LO + self.lo1, 0), self.part(z * LO + self.lo2, 1)
        return [
            remote(first, first, self.send.at[0], self.far.at[z], self.hi * LO + self.lo2, self.c),
            remote(last, last, self.send.at[0], self.far.at[z], self.hi * LO + self.lo1, self.c),
        ]

    def arrived(self, ref, sem):
        remote(ref, ref, self.send.at[0], sem, self.s, 1 - self.c).wait_recv()

    def wait_own(self, z):
        self.arrived(self.full(z * LO + self.lo), self.own.at[z])

    def wait_direct(self, z):
        self.arrived(self.blocks(2), self.near.at[z])

    def wait_diag(self, z):
        self.arrived(self.full(z * LO + self.lo3), self.far.at[z])

    def wait_sent(self, planes):
        ref = self.blocks(3 * planes)
        remote(ref, ref, self.send.at[0], self.far.at[0], self.s, 1 - self.c).wait_send()


def start(copies):
    for copy in copies:
        copy.start()


def scoped(name, fn, *args):
    with jax.named_scope(name):
        return fn(*args)


def layer_kernel(HI, G, NC, names, *refs):
    r = Refs(names, refs)
    s = lax.axis_index("sp")
    c = lax.axis_index("tp")
    hi = s // LO
    lo = s % LO
    lo1 = lo + 1 - 2 * (lo % 2)
    lo2 = (lo + 2) % LO
    lo3 = (lo1 + 2) % LO
    other = 1 - c
    peers = (lo1, lo2, lo3)
    T = r.q_v.shape[0]
    H = T // 2
    D = r.tok_v.shape[1]
    R = r.up_v.shape[0]
    CH = r.up_buf.shape[1]
    W = r.dn_v.shape[1]
    PL = LO * T
    QR = 2 * PL
    own_cols = pl.ds(pl.multiple_of(hi * CH, LANES), CH)
    own_lanes = pl.ds(pl.multiple_of(lo * LANES, LANES), LANES)

    barrier = pltpu.get_barrier_semaphore()
    for p in peers:
        pl.semaphore_signal(barrier, inc=1, device_id={"sp": hi * LO + p, "tp": c}, device_id_type=MESH)
    pl.semaphore_signal(barrier, inc=1, device_id={"sp": s, "tp": other}, device_id_type=MESH)
    for dz in range(1, HI):
        far = ((hi + dz) % HI) * LO + lo
        pl.semaphore_signal(barrier, inc=1, device_id={"sp": far, "tp": c}, device_id_type=MESH)
    local = [
        (r.bias_hbm, r.bias_v),
        (r.kv_hbm, r.kv_v),
        (r.q_hbm, r.q_v),
        (r.up_hbm, r.up_v),
        (r.dn_hbm, r.dn_v),
        (r.up_hbm.at[:, own_cols], r.up_buf.at[pl.ds(s * R, R)]),
        (r.dn_hbm.at[pl.ds(hi * CH, CH)], r.dn_buf.at[s]),
        (r.tok_hbm, r.tok_v),
        (r.wo_hbm, r.wo_v),
        (r.gain_hbm, r.gain_v),
    ]
    loads = [pltpu.make_async_copy(a, b, r.load_sem.at[i]) for i, (a, b) in enumerate(local)]
    start(loads[:5])
    loads[0].wait()

    half_lane = lax.broadcasted_iota(jnp.int32, (2 * G, LANES), 1) // HEAD
    bias = r.bias_v[...].astype(F32)
    bias = jnp.where(half_lane == lo % 2, jnp.concatenate([bias, bias], axis=1), 0.0)
    for g in range(G):
        r.bias_out[g] = bias[2 * g : 2 * g + 2]
    with jax.named_scope("barrier"):
        for load in loads[1:3]:
            load.wait()
        pl.semaphore_wait(barrier, 4 + (HI - 1))

    place = (s, c, hi, lo, lo1, lo2, lo3)
    up = Piece(
        place,
        lambda j, a, n: r.up_buf.at[pl.ds(j * R + a, n)],
        lambda n: r.up_buf.at[pl.ds(0, n * R)],
        R,
        (r.up_sp, r.up_own, r.up_near, r.up_diag),
    )
    dn = Piece(
        place,
        lambda j, a, n: r.dn_buf.at[j, pl.ds(a, n)],
        lambda n: r.dn_buf.at[pl.ds(0, n)],
        CH,
        (r.dn_sp, r.dn_own, r.dn_near, r.dn_diag),
    )

    def arrived(ref, sem):
        remote(ref, ref, r.pj_send, sem, s, other).wait_recv()

    def sent(ref, sem):
        remote(ref, ref, sem, r.pj_recv, s, other).wait_send()

    def send_keys(d, p):
        lanes = pl.ds(pl.multiple_of(p * LANES, LANES), LANES)
        dev = (hi + d) * LO + p
        return [
            remote(r.kv_v.at[:, lanes], r.kv_buf.at[hi, pl.ds(lo * T, T)], r.k_send.at[d], r.k_recv.at[hi], dev, c),
            remote(r.bias_out.at[p], r.bias_in.at[hi, lo], r.b_send.at[d], r.b_recv.at[hi], dev, c),
        ]

    def send_queries(p):
        lanes = pl.ds(pl.multiple_of(p * LANES, LANES), LANES)
        return remote(r.q_v.at[:, lanes], r.q_in.at[lo], r.q_send.at[0], r.q_recv.at[0], hi * LO + p, c)

    def keys_of(z, shards):
        arrived(r.kv_buf.at[z, pl.ds(0, shards * T)], r.k_recv.at[z])
        arrived(r.bias_in.at[z, pl.ds(0, shards)], r.b_recv.at[z])

    def join_bias(z):
        for i in range(LO // 2):
            r.bias_pl[z, :, i * LANES : (i + 1) * LANES] = r.bias_in[z, 2 * i] + r.bias_in[z, 2 * i + 1]

    def up_far(hp):
        cols = pl.ds(pl.multiple_of(hp * CH, LANES), CH)
        return remote(r.up_v.at[:, cols], up.full(s), r.wz_send.at[0], r.up_own.at[hi], hp * LO + lo, c)

    def dn_far(hp):
        rows = pl.ds(hp * CH, CH)
        return remote(r.dn_v.at[rows], dn.full(s), r.wz_send.at[1], r.dn_own.at[hi], hp * LO + lo, c)

    small = jnp.minimum(hi, HI - 1 - hi)
    tilt = jnp.where(hi <= HI - 1 - hi, 1, -1)

    def nth(k):
        if k == 0:
            return hi
        near = hi + (k + 1) // 2 if k % 2 else hi - k // 2
        return jnp.where(k <= 2 * small, near, hi + tilt * (k - small))

    upper = hi // (HI // 2)
    rank = hi + upper * (HI - 1 - 2 * hi)

    def order(k):
        if k == 0:
            return hi
        z = k - 1 + (rank < k).astype(jnp.int32)
        return z + upper * (HI - 1 - 2 * z)

    def below(far, d):
        @pl.when(hi >= d)
        def _():
            far(hi - d).start()

    def above(far, d):
        @pl.when(hi + d < HI)
        def _():
            far(hi + d).start()

    for p in peers:
        pl.semaphore_signal(r.ready, inc=1, device_id={"sp": hi * LO + p, "tp": c}, device_id_type=MESH)
    for p in peers:
        start(send_keys(0, p))
        send_queries(p).start()

    def raise_keys(shards):
        for d in range(HI - 1, 0, -1):

            @pl.when(hi + d < HI)
            def _():
                for p in shards:
                    start(send_keys(d, p))

    raise_keys((lo,))
    start(loads[5:])
    for load in loads[3:5]:
        load.wait()
    pair = hi + 1 - 2 * (hi % 2)
    for d in range(1, HI):
        below(up_far, d)
        if d == 1:
            pl.when(hi % 2 == 1)(lambda: dn_far(pair).start())
    scoped("ready", pl.semaphore_wait, r.ready, LO - 1)
    raise_keys(peers)
    start(up.direct(hi, r.up_v.at[:, own_cols]))
    for d in range(1, HI):
        above(up_far, d)
        if d == 1:
            pl.when(hi % 2 == 0)(lambda: dn_far(pair).start())
    start(dn.direct(hi, r.dn_v.at[pl.ds(hi * CH, CH)]))

    r.q_in[lo] = r.q_v[:, own_lanes]
    r.kv_buf[hi, pl.ds(lo * T, T), :] = r.kv_v[:, own_lanes]
    r.bias_in[hi, lo] = r.bias_out[lo]
    row_id = lax.broadcasted_iota(jnp.int32, (PL, PL + LANES), 0)
    col_id = lax.broadcasted_iota(jnp.int32, (PL, PL + LANES), 1)
    after_key = (row_id > col_id) | (col_id >= PL)
    r.tri_buf[...] = jnp.where(after_key, 1.0, 0.0).astype(BF16)
    low = lax.broadcasted_iota(jnp.int32, (T, LANES), 1) < HEAD

    with jax.named_scope("heads_wait"):
        keys_of(hi, LO - 1)
        arrived(r.q_in.at[pl.ds(0, LO - 1)], r.q_recv.at[0])
    join_bias(hi)
    for j in range(LO):
        qg = r.q_in[j].astype(F32) * 0.125
        r.q_all[j * T : (j + 1) * T] = jnp.where(low, qg, 0.0).astype(BF16)
        r.q_all[PL + j * T : PL + (j + 1) * T] = jnp.where(low, pltpu.roll(qg, HEAD, 1), 0.0).astype(BF16)

    step = 128

    def attend(z, own):
        keys = r.kv_buf[z]
        for i in range(QR // step):
            rows = slice(i * step, (i + 1) * step)
            head = i * step // PL
            scores = dot_nt(r.q_all[rows], keys) + r.bias_pl[z, head : head + 1, :]
            soft = jnp.maximum(scores, 0.0) + jnp.log(1.0 + jnp.exp(-jnp.abs(scores)))
            log_pass = -soft
            if own:
                query = i * step % PL + lax.broadcasted_iota(jnp.int32, (step, PL), 0)
                strict = lax.broadcasted_iota(jnp.int32, (step, PL), 1) < query
                log_pass = jnp.where(strict, log_pass, 0.0)
            top = log_pass.astype(BF16)
            rest = (log_pass - top.astype(F32)).astype(BF16)
            sums = jnp.dot(top, r.tri_buf[...], preferred_element_type=F32) + jnp.dot(
                rest, r.tri_buf[...], preferred_element_type=F32
            )
            power = scores - soft + sums[:, :PL]
            if not own:
                held = r.carry[rows]
                power = power + jnp.concatenate([held] * (PL // LANES), axis=1)
            weights = jnp.exp(power)
            if own:
                weights = jnp.where(strict, weights, 0.0)
            part = jnp.dot(weights.astype(BF16), keys, preferred_element_type=F32)
            if own:
                r.acc[rows] = part
                r.carry[rows] = sums[:, PL:]
            else:
                r.acc[rows] += part
                r.carry[rows] = held + sums[:, PL:]

    def look(d):
        @pl.when(hi >= d)
        def _():
            z = hi - d
            scoped(f"keys_wait{d}", keys_of, z, LO)
            join_bias(z)
            scoped(f"attend{d}", attend, z, False)

    def relay_direct(piece, k):
        z = nth(k) if piece is up else order(k)
        scoped(f"{'UD'[piece is dn]}own_wait{k}", piece.wait_own, z)
        start(piece.direct(z))

    def relay_diag(piece, k):
        z = nth(k) if piece is up else order(k)
        scoped(f"{'UD'[piece is dn]}direct_wait{k}", piece.wait_direct, z)
        start(piece.diag(z))

    scoped("attend0", attend, hi, True)
    relay_diag(up, 0)
    for d in range(1, HI):
        look(d)
        if d == 1:
            relay_direct(up, 1)

    heads = [r.acc[h * PL : (h + 1) * PL] for h in range(2)]
    low_pl = lax.broadcasted_iota(jnp.int32, (PL, LANES), 1) < HEAD
    r.att_pl[...] = jnp.where(low_pl, pltpu.roll(heads[0], HEAD, 1), heads[1]).astype(BF16)

    def att_back(p):
        src = r.att_pl.at[pl.ds(p * T, T)]
        return remote(src, r.att_buf.at[:, own_lanes], r.t_send.at[0], r.t_recv.at[0], hi * LO + p, c)

    for p in peers:
        att_back(p).start()

    def dn_below():
        for d in range(1, HI):

            @pl.when((hi >= d) & (hi - d != pair))
            def _():
                dn_far(hi - d).start()

    def dn_above():
        for d in range(1, HI):

            @pl.when((hi + d < HI) & (hi + d != pair))
            def _():
                dn_far(hi + d).start()

    dn_below()
    pl.when(hi == 0)(dn_above)
    r.att_buf[:, own_lanes] = r.att_pl[pl.ds(lo * T, T), :]
    relay_diag(dn, 0)
    pl.when(upper == 0)(lambda: relay_direct(up, 2))
    with jax.named_scope("att_wait"):
        for load in loads[5:]:
            load.wait()
        arrived(r.att_pl.at[pl.ds(0, (LO - 1) * T)], r.t_recv.at[0])

    att = r.att_buf[...]
    wide = 512 if D % 512 == 0 else LANES
    for i in range(D // wide):
        cols = slice(i * wide, (i + 1) * wide)
        r.pj_buf[:, cols] = jnp.dot(att, r.wo_v[:, cols], preferred_element_type=F32).astype(BF16)
    pj_copy = remote(r.pj_buf.at[pl.ds(other * H, H)], r.pj_in, r.pj_send, r.pj_recv, s, other)
    pj_copy.start()
    pl.when(hi > 0)(dn_above)
    relay_diag(up, 1)
    relay_direct(dn, 1)
    pl.when(upper == 1)(lambda: relay_direct(up, 2))
    scoped("pj_wait", pj_copy.wait)
    mine = pl.ds(c * H, H)
    total = r.pj_buf[mine, :].astype(F32) + r.pj_in[...].astype(F32)
    residual = (r.tok_v[mine, :].astype(F32) + total).astype(BF16)
    r.res_buf[...] = residual
    values = residual.astype(F32)
    factor = lax.rsqrt(jnp.mean(values * values, axis=-1, keepdims=True) + EPSILON)
    r.n_buf[pl.ds((c * HI + hi) * H, H), :] = (values * factor * r.gain_v[...]).astype(BF16)

    NW = D // NC

    def n_at(z, core, q):
        return r.n_buf.at[pl.ds((core * HI + z) * H, H), q * NW : (q + 1) * NW]

    def n_up(z, q):
        return remote(n_at(z, c, q), n_at(z, c, q), r.nu_send.at[z], r.nz_recv.at[z * NC + q], s + LO, c)

    def n_down(z, q):
        return remote(n_at(z, c, q), n_at(z, c, q), r.nd_send.at[z], r.nz_recv.at[z * NC + q], s - LO, c)

    def n_pass(z, q):
        return remote(n_at(z, c, q), n_at(z, c, q), r.np_send.at[0], r.nc_recv.at[0], s, other)

    for q in range(NC):

        @pl.when(hi + 1 < HI)
        def _():
            n_up(hi, q).start()

        @pl.when(hi > 0)
        def _():
            n_down(hi, q).start()

    for q in range(NC):
        n_pass(hi, q).start()

    def norm_take(k):
        z = order(k)
        for q in range(NC):
            scoped(f"norm_wait{k}", arrived, n_at(z, c, q), r.nz_recv.at[z * NC + q])

            @pl.when((z < hi) & (hi + 1 < HI))
            def _():
                n_up(z, q).start()

            @pl.when((z > hi) & (hi > 0))
            def _():
                n_down(z, q).start()

            n_pass(z, q).start()

    relay_direct(up, 3)
    relay_diag(up, 2)
    relay_diag(dn, 1)
    norm_take(1)
    relay_diag(up, 3)
    relay_direct(dn, 2)
    norm_take(2)
    relay_direct(dn, 3)
    norm_take(3)
    relay_diag(dn, 2)
    half = HI * H
    wide = 256 if CH % 256 == 0 else LANES

    def hide(core):
        rows = pl.ds(pl.multiple_of(core * half, half), half)
        for i in range(CH // wide):
            cols = slice(i * wide, (i + 1) * wide)
            raw = jnp.maximum(jnp.dot(r.n_buf[rows, :], r.up_buf[:, cols], preferred_element_type=F32), 0.0)
            r.hid_buf[rows, cols] = (raw * raw).astype(BF16)

    with jax.named_scope("up_wait"):
        for k in range(HI):
            up.wait_diag(nth(k))
    hide(c)
    with jax.named_scope("norm_other_wait"):
        arrived(r.n_buf.at[pl.ds(0, HI * H)], r.nc_recv.at[0])
    hide(other)

    CW = LO * W
    mine_rows = pl.ds(c * half, half)

    def x_out(k):
        z = order(k)
        rows = pl.ds(other * half, half)
        return remote(r.ps_buf.at[z, rows], r.x_in.at[z], r.x_send.at[0], r.x_recv.at[z], s, other)

    edge = (hi == 0) | (hi == HI - 1)
    near = hi + 1 - 2 * (hi % 2)
    away = (1 - upper) * (HI - 1)
    middle = away + 2 * upper - 1

    def p_out(z, hp):
        return remote(r.xs_buf.at[z, pl.ds(hp * H, H)], r.pr_buf.at[z, hi], r.p_send.at[0], r.p_recv.at[z], hp * LO + lo, c)

    def spread(k):
        z = order(k)
        scoped(f"x_wait{k}", arrived, r.x_in.at[z], r.x_recv.at[z])
        mixed = r.ps_buf[z, mine_rows, :].astype(F32) + r.x_in[z].astype(F32)
        r.xs_buf[z] = mixed.astype(BF16)

        p_out(z, away).start()
        p_out(z, middle).start()
        pl.when(jnp.logical_not(edge))(lambda: p_out(z, near).start())

    for k in range(HI):
        z = order(k)
        scoped(f"dn_wait{k}", dn.wait_diag, z)
        for q in range(0, LO, 2):
            pair = jnp.concatenate([r.dn_buf[z * LO + q], r.dn_buf[z * LO + q + 1]], axis=1)
            part = jnp.dot(r.hid_buf[...], pair, preferred_element_type=F32)
            r.ps_buf[z, :, q * W : (q + 2) * W] = part.astype(BF16)
        x_out(k).start()
        if k > 0:
            spread(k - 1)
        if k == 1:
            relay_diag(dn, HI - 1)
    spread(HI - 1)

    @pl.when(edge)
    def _():
        for k in range(HI):
            p_out(order(k), near).start()

    def drain():
        for z in range(1, HI):

            @pl.when(hi + z < HI)
            def _():
                sent(r.kv_buf.at[0], r.k_send.at[z])
                sent(r.bias_in.at[0], r.b_send.at[z])

        sent(r.kv_buf.at[0, pl.ds(0, (LO - 1) * T)], r.k_send.at[0])
        sent(r.bias_in.at[0, pl.ds(0, LO - 1)], r.b_send.at[0])
        sent(r.q_in.at[pl.ds(0, LO - 1)], r.q_send.at[0])
        sent(r.att_pl.at[pl.ds(0, (LO - 1) * T)], r.t_send.at[0])
        sent(up.blocks(HI - 1), r.wz_send.at[0])
        sent(dn.blocks(HI - 1), r.wz_send.at[1])
        up.wait_sent(HI)
        dn.wait_sent(HI)
        for z in range(HI):

            @pl.when((z <= hi) & (hi + 1 < HI))
            def _():
                sent(r.res_buf, r.nu_send.at[z])

            @pl.when((z >= hi) & (hi > 0))
            def _():
                sent(r.res_buf, r.nd_send.at[z])

        sent(r.n_buf.at[pl.ds(0, HI * H)], r.np_send.at[0])
        sent(r.x_in, r.x_send.at[0])

    scoped("drain", drain)
    for k in range(HI):
        z = order(k)
        cols = pl.ds(pl.multiple_of(z * CW, LANES), CW)
        update = r.xs_buf[z, pl.ds(hi * H, H), :].astype(F32)
        scoped(f"sum_wait{k}", arrived, r.pr_buf.at[z, pl.ds(0, HI - 1)], r.p_recv.at[z])
        for far in range(1, HI):
            update = update + r.pr_buf[z, (hi + far) % HI].astype(F32)
        r.out_ref[:, cols] = (r.res_buf[:, cols].astype(F32) + update).astype(BF16)
    sent(r.pr_buf.at[:, pl.ds(0, HI - 1)], r.p_send.at[0])


def fits(tokens, queries, key_values, stop_bias, up_proj, down_proj):
    sp = lax.axis_size("sp")
    rows, seqs, heads = stop_bias.shape
    hidden = up_proj.shape[1]
    return (
        lax.axis_size("tp") == 2
        and sp == LO * LO
        and seqs == 1
        and heads == 2 * LO
        and queries.shape[2] == heads * HEAD
        and key_values.shape[2] == heads * HEAD
        and 2 * HEAD == LANES
        and 2 * rows == LANES
        and hidden % (sp // LO * LANES) == 0
        and down_proj.shape[1] % LANES == 0
        and up_proj.shape[0] % 16 == 0
        and tokens.shape[2] % 512 == 0
    )


def body(tokens, queries, key_values, stop_bias, out_proj, norm_gain, up_proj, down_proj):
    if not fits(tokens, queries, key_values, stop_bias, up_proj, down_proj):
        return general_body(
            tokens, queries, key_values, stop_bias, out_proj, norm_gain, up_proj, down_proj
        )
    sp = lax.axis_size("sp")
    HI = sp // LO
    T, _, D = tokens.shape
    H = T // 2
    heads = stop_bias.shape[2]
    G = heads // 2
    R, hidden = up_proj.shape
    CH = hidden // HI
    W = down_proj.shape[1]
    PL = LO * T
    NC = 4
    vmem = pl.BlockSpec(memory_space=pltpu.VMEM)
    hbm = pl.BlockSpec(memory_space=pl.ANY)

    def sem(*shape):
        return pltpu.SemaphoreType.DMA(shape)

    operands = dict(
        tok_hbm=(tokens.reshape(T, D), hbm),
        q_hbm=(queries.reshape(T, queries.shape[2]), hbm),
        kv_hbm=(key_values.reshape(T, key_values.shape[2]), hbm),
        bias_hbm=(stop_bias.reshape(T, heads).T, hbm),
        wo_hbm=(out_proj, hbm),
        gain_hbm=(norm_gain.reshape(1, D), hbm),
        up_hbm=(up_proj, hbm),
        dn_hbm=(down_proj, hbm),
    )
    scratch = dict(
        tok_v=pltpu.VMEM((T, D), BF16),
        bias_v=pltpu.VMEM((heads, T), BF16),
        q_v=pltpu.VMEM((T, G * LANES), BF16),
        kv_v=pltpu.VMEM((T, G * LANES), BF16),
        wo_v=pltpu.VMEM(out_proj.shape, BF16),
        gain_v=pltpu.VMEM((1, D), F32),
        up_v=pltpu.VMEM((R, hidden), BF16),
        dn_v=pltpu.VMEM((hidden, W), BF16),
        up_buf=pltpu.VMEM((sp * R, CH), BF16),
        dn_buf=pltpu.VMEM((sp, CH, W), BF16),
        bias_out=pltpu.VMEM((G, 2, LANES), F32),
        bias_in=pltpu.VMEM((HI, LO, 2, LANES), F32),
        bias_pl=pltpu.VMEM((HI, 2, PL), F32),
        q_in=pltpu.VMEM((LO, T, LANES), BF16),
        q_all=pltpu.VMEM((2 * PL, LANES), BF16),
        kv_buf=pltpu.VMEM((HI, PL, LANES), BF16),
        tri_buf=pltpu.VMEM((PL, PL + LANES), BF16),
        carry=pltpu.VMEM((2 * PL, LANES), F32),
        acc=pltpu.VMEM((2 * PL, LANES), F32),
        att_pl=pltpu.VMEM((PL, LANES), BF16),
        att_buf=pltpu.VMEM((T, G * LANES), BF16),
        pj_buf=pltpu.VMEM((T, D), BF16),
        pj_in=pltpu.VMEM((H, D), BF16),
        res_buf=pltpu.VMEM((H, D), BF16),
        n_buf=pltpu.VMEM((HI * T, D), BF16),
        hid_buf=pltpu.VMEM((HI * T, CH), BF16),
        ps_buf=pltpu.VMEM((HI, HI * T, LO * W), BF16),
        x_in=pltpu.VMEM((HI, HI * H, LO * W), BF16),
        xs_buf=pltpu.VMEM((HI, HI * H, LO * W), BF16),
        pr_buf=pltpu.VMEM((HI, HI, H, LO * W), BF16),
        load_sem=sem(10),
        k_send=sem(HI),
        b_send=sem(HI),
        ready=pltpu.SemaphoreType.REGULAR,
        q_send=sem(1),
        k_recv=sem(HI),
        b_recv=sem(HI),
        q_recv=sem(1),
        wz_send=sem(2),
        up_sp=sem(1),
        up_own=sem(HI),
        up_near=sem(HI),
        up_diag=sem(HI),
        dn_sp=sem(1),
        dn_own=sem(HI),
        dn_near=sem(HI),
        dn_diag=sem(HI),
        t_send=sem(1),
        t_recv=sem(1),
        pj_send=pltpu.SemaphoreType.DMA,
        pj_recv=pltpu.SemaphoreType.DMA,
        nu_send=sem(HI),
        nd_send=sem(HI),
        np_send=sem(1),
        nz_recv=sem(HI * NC),
        nc_recv=sem(1),
        x_send=sem(1),
        x_recv=sem(HI),
        p_send=sem(1),
        p_recv=sem(HI),
    )
    names = [*operands, "out_ref", *scratch]
    out = pl.pallas_call(
        lambda *refs: layer_kernel(HI, G, NC, names, *refs),
        out_shape=pltpu.VMEM((H, D), BF16),
        in_specs=[spec for _, spec in operands.values()],
        out_specs=vmem,
        scratch_shapes=list(scratch.values()),
        compiler_params=pltpu.CompilerParams(
            collective_id=0, has_side_effects=True, vmem_limit_bytes=56 * 1024 * 1024
        ),
        name="layer",
    )(*[value for value, _ in operands.values()])
    return out.reshape(H, 1, D)


def solution(mesh):
    return jax.shard_map(
        body,
        mesh=mesh,
        in_specs=(
            P("sp", None, None),
            P("sp", None, "tp"),
            P("sp", None, "tp"),
            P("sp", None, "tp"),
            P("tp", None),
            P(),
            P("sp", "tp"),
            P("tp", "sp"),
        ),
        out_specs=P(("sp", "tp"), None, None),
        check_vma=False,
    )
```
